32 devices in a mesh: row: 8 (over z, x), col: 4 (over y, core).
Axes of the slice: x: 2, y: 2, z: 4, core: 2. Of those that a mesh axis runs over, the one named last changes fastest.
Arguments:
- tokens: bfloat16 [8192, 2048], P('row'), may hold values from -136 to 136
- norm_gain: float32 [2048], replicated, may hold values from 0.1 to 1.9
- w_in: bfloat16 [2048, 1024], P(None, 'col'), may hold values from -0.125 to 0.125
- w_out: bfloat16 [1024, 2048], P(None, 'col'), may hold values from -0.1875 to 0.1875
Outputs:
- mixed_tokens: bfloat16 [8192, 2048], P('row', 'col')
The draws below stay inside these ranges and needn't reach their ends.
All inputs are finite; a program needn't handle non-finite values.
Results may differ from the reference program's by a relative error of at most 0.013.
Values may be sent and summed in bfloat16 or wider, within the bound.
A program may use at most 64 MiB of HBM per device.

```python
import math
import jax
import jax.numpy as jnp
from jax import lax

D = 2048
FW = 1024
GROUP = 256
GROUPS = 4
LENGTH = 8192


def draw_tokens(key, part):
    key_values, key_scales = jax.random.split(key, 2)
    columns = jnp.arange(D, dtype=jnp.float32) / D
    values = jnp.clip(jax.random.normal(key_values, (LENGTH, D), jnp.float32), -6.0, 6.0)
    row_scale = jnp.exp(jax.random.uniform(key_scales, (LENGTH, 1), jnp.float32, 0.0, 0.2))
    col_scale = jnp.exp(columns * math.log(4.0))
    return (values * row_scale * col_scale[None, :]).astype(jnp.bfloat16)


def level_of(own_key, extent, cuts, smallest, high):
    factor_of, own = 1.0, jax.random.fold_in(own_key, 6)
    for position, shards_of in cuts:
        steps = jnp.exp(jax.random.uniform(jax.random.fold_in(own, position), (shards_of,), jnp.float32, smallest / len(cuts), high / len(cuts)))
        factor_of = factor_of * jnp.repeat(steps, extent[position] // shards_of).reshape([-1 if axis == position else 1 for axis in range(len(extent))])
    return factor_of


def bell_draw(rng, dims, spread, most, cuts=(), kind=jnp.bfloat16):
    drawn = jax.random.normal(rng, dims, jnp.float32) * spread
    if len(cuts) > 0:
        drawn = level_of(rng, dims, cuts, -0.22, 0.18) * drawn
    return jnp.clip(drawn, min=-most, max=most).astype(kind)


def setup_inputs(seed: int = 0) -> dict:
    keys = jax.random.split(jax.random.key(seed), 5)
    tokens = draw_tokens(jax.random.fold_in(keys[4], 71), 0)
    norm_gain = jnp.clip(1.0 + 0.18 * jax.random.normal(keys[1], (D,), jnp.float32), 0.1, 1.9)
    w_in = bell_draw(keys[2], (D, FW), D ** -0.5, 0.125, ((1, 4),))
    w_out = bell_draw(keys[3], (FW, D), FW ** -0.5, 0.1875, ((1, 4),))
    return {"tokens": tokens, "norm_gain": norm_gain, "w_in": w_in, "w_out": w_out}


NORM_EPS = 1e-06

def reference(tokens, norm_gain, w_in, w_out):
    widened = tokens.astype(jnp.float32)
    inverse = lax.rsqrt(lax.optimization_barrier(jnp.mean(widened * widened, axis=1, keepdims=True)) + NORM_EPS)
    normed = (widened * inverse * norm_gain[None, :]).astype(jnp.bfloat16)
    projected = jnp.dot(normed, w_in, preferred_element_type=jnp.float32).astype(jnp.bfloat16)
    grouped = projected.astype(jnp.float32).reshape(LENGTH, GROUPS, GROUP)
    spectrum = jnp.real(jnp.fft.fftn(grouped, axes=(0, 2), norm='ortho'))
    spectral = spectrum.reshape(LENGTH, FW).astype(jnp.bfloat16)
    return jnp.dot(spectral, w_out, preferred_element_type=jnp.float32).astype(jnp.bfloat16)
```

```python
import functools
import math

import jax
import jax.numpy as jnp
import numpy as np
from jax import lax
from jax.experimental import pallas as pl
from jax.experimental.pallas import tpu as pltpu
from jax.sharding import PartitionSpec as P

GROUP = 256


NORM_EPS = 1e-06


def as_sent(array):

    def short(part):
        return part.astype(jnp.bfloat16) if part.dtype == jnp.float32 else part

    return jax.tree.map(short, array)


def rotation_table(first_index, second_index, spectral_magnitude, factor):
    phase = (first_index * second_index % spectral_magnitude).astype(jnp.float32) * (
        2.0 * math.pi / spectral_magnitude
    )
    return (jnp.cos(phase) * factor, jnp.sin(phase) * factor)


def twiddle(real_input_values, imag_in, freq_index, pos_index, spectral_magnitude):
    cosine, sine = rotation_table(freq_index, pos_index, spectral_magnitude, 1.0)
    return (
        real_input_values * cosine + imag_in * sine,
        imag_in * cosine - real_input_values * sine,
    )


def second_section(stacked, half):
    length_dev = stacked.shape[1]
    stride = min(length_dev, 512)
    positions = lax.broadcasted_iota(jnp.int32, (length_dev, stride), 0)
    real_blocks = []
    imag_blocks = []
    for offset in range(0, length_dev, stride):
        freqs = lax.broadcasted_iota(jnp.int32, (length_dev, stride), 1) + offset
        cosine, sine = rotation_table(positions, freqs, length_dev, 1.0)
        with_cos = jnp.dot(stacked, cosine, precision=lax.Precision.HIGH)
        with_sin = jnp.dot(stacked, sine, precision=lax.Precision.HIGH)
        real_blocks.append(with_cos[:half] + with_sin[half:])
        imag_blocks.append(with_cos[half:] - with_sin[:half])
    return (jnp.concatenate(real_blocks, 1), jnp.concatenate(imag_blocks, 1))


def reorder_positions(arrived):
    channels, row_count, _, block_len = arrived.shape
    return jnp.swapaxes(arrived.reshape(channels, row_count, block_len), 1, 2).reshape(
        channels, row_count * block_len
    )


def local(tokens, norm_gain, w_in, w_out):
    length_dev = tokens.shape[0]
    row_count = lax.axis_size("row")
    col_count = lax.axis_size("col")
    total_len = length_dev * row_count
    widened = tokens.astype(jnp.float32)
    inverse = lax.rsqrt(jnp.mean(widened * widened, axis=1, keepdims=True) + NORM_EPS)
    normed = (widened * inverse * norm_gain[None, :]).astype(jnp.bfloat16)
    projected = lax.dot_general(
        w_in, normed, (((0,), (1,)), ((), ())), preferred_element_type=jnp.float32
    ).astype(jnp.bfloat16)
    channels = projected.shape[0]
    block_len = length_dev // row_count
    small_cos, small_sin = rotation_table(
        lax.broadcasted_iota(jnp.int32, (row_count, row_count), 0),
        lax.broadcasted_iota(jnp.int32, (row_count, row_count), 1),
        row_count,
        1.0 / math.sqrt(total_len),
    )
    per_row = channels // row_count
    arrived = lax.all_to_all(
        projected.reshape(channels, 1, length_dev), "row", split_axis=0, concat_axis=1, tiled=True
    )
    values = arrived.astype(jnp.float32)
    real_one = jnp.einsum("ka,cab->ckb", small_cos, values, precision=lax.Precision.HIGH)
    imag_one = -jnp.einsum("ka,cab->ckb", small_sin, values, precision=lax.Precision.HIGH)
    freq_index = lax.broadcasted_iota(jnp.int32, (row_count, length_dev), 0)
    pos_index = lax.broadcasted_iota(jnp.int32, (row_count, length_dev), 1)
    real_two, imag_two = twiddle(real_one, imag_one, freq_index, pos_index, total_len)
    stacked = jnp.concatenate(
        [
            real_two.reshape(per_row * row_count, length_dev),
            imag_two.reshape(per_row * row_count, length_dev),
        ],
        0,
    )
    real_three, imag_three = second_section(stacked, per_row * row_count)
    shaped = (per_row, row_count, row_count, block_len)
    back_real, back_imag = (
        lax.all_to_all(
            real_three.reshape(shaped).astype(jnp.bfloat16),
            "row",
            split_axis=2,
            concat_axis=0,
            tiled=True,
        ).astype(jnp.float32),
        lax.all_to_all(
            imag_three.reshape(shaped).astype(jnp.bfloat16),
            "row",
            split_axis=2,
            concat_axis=0,
            tiled=True,
        ).astype(jnp.float32),
    )
    spec_real = reorder_positions(back_real)
    spec_imag = reorder_positions(back_imag)
    quarter = length_dev // col_count
    group_cosine_table, group_sine_table = rotation_table(
        lax.broadcasted_iota(jnp.int32, (GROUP, GROUP), 0),
        lax.broadcasted_iota(jnp.int32, (GROUP, GROUP), 1),
        GROUP,
        1.0 / math.sqrt(GROUP),
    )
    real_input_values = lax.all_to_all(
        as_sent(spec_real.reshape(channels, col_count, quarter)),
        "col",
        split_axis=1,
        concat_axis=0,
        tiled=True,
    )
    imag_in = lax.all_to_all(
        as_sent(spec_imag.reshape(channels, col_count, quarter)),
        "col",
        split_axis=1,
        concat_axis=0,
        tiled=True,
    )
    width_all = real_input_values.shape[0]
    item_count = real_input_values.shape[2]
    groups = width_all // GROUP
    real_by_group = real_input_values.reshape(groups, GROUP, item_count)
    imaginary_by_group = imag_in.reshape(groups, GROUP, item_count)
    merged_spectrum = jnp.einsum(
        "hz,azo->aho", group_cosine_table, real_by_group, precision=lax.Precision.HIGH
    )
    merged_spectrum = merged_spectrum + jnp.einsum(
        "hz,azo->aho", group_sine_table, imaginary_by_group, precision=lax.Precision.HIGH
    )
    result = merged_spectrum.reshape(width_all, 1, item_count).astype(jnp.bfloat16)
    spectral = lax.all_to_all(result, "col", split_axis=0, concat_axis=1, tiled=True)
    output = lax.dot_general(
        lax.all_gather(spectral.reshape(channels, length_dev), "col", axis=0, tiled=True),
        w_out,
        (((0,), (0,)), ((), ())),
        preferred_element_type=jnp.float32,
    )
    return output.astype(jnp.bfloat16)


HALVES = 2
POINTS = 8
SPLIT = 1
LANES = 128
MESH = pl.DeviceIdType.MESH


def channel_tables(group, total_len):
    half = group // 2
    index = np.arange(group)
    angle = 2.0 * np.pi * (index[:, None] * index[None, :] % group) / group
    transform = np.concatenate([np.cos(angle[: half + 1]), np.sin(angle[1:half])], 0)
    fold = np.zeros((group, group))
    for k in range(half + 1):
        fold[k, k] = 1.0
        fold[k, -k % group] = 1.0
    for k in range(1, half):
        fold[half + k, group - k] = 1.0
        fold[half + k, k] = -1.0
    return (transform / math.sqrt(group)).astype(jnp.bfloat16), fold.astype(jnp.bfloat16)


def position_tables(block, total_len):
    j = np.arange(block)
    angle = 2.0 * np.pi * (np.arange(POINTS)[:, None] * j[None, :]) / total_len
    twiddles = np.stack([np.cos(angle), np.sin(angle)]).astype(np.float32)
    root = 32
    coarse = 2.0 * np.pi * (np.arange(block // root)[:, None] * root * j[None, :] % block) / block
    fine = 2.0 * np.pi * (np.arange(root)[:, None] * j[None, :] % block) / block
    scale = 1.0 / math.sqrt(total_len)
    coarse = np.stack([np.cos(coarse), np.sin(coarse)]).astype(np.float32)
    fine = np.stack([np.cos(fine) * scale, np.sin(fine) * scale]).astype(np.float32)
    return twiddles, coarse, fine


def eight_points(x):
    a = [x[i] + x[i + 4] for i in range(4)]
    b = [x[i] - x[i + 4] for i in range(4)]
    even, odd = a[0] + a[2], a[1] + a[3]
    root = math.sqrt(0.5)
    minus, plus = root * (b[1] - b[3]), root * (b[1] + b[3])
    one = (b[0] + minus, -b[2] - plus)
    two = (a[0] - a[2], a[3] - a[1])
    three = (b[0] - minus, b[2] - plus)
    return [
        (even + odd, None),
        one,
        two,
        three,
        (even - odd, None),
        (three[0], -three[1]),
        (two[0], -two[1]),
        (one[0], -one[1]),
    ]


def mixer_kernel(
    steps, ahead,
    tokens_hbm, gain_hbm, w_in_hbm, w_out_hbm, forward_hbm, fold_hbm, twiddle_hbm, coarse_hbm, fine_hbm,
    out_ref,
    tokens, gain, w_in, w_out, forward, fold, twiddles, coarse, fine,
    packed, arrived, stage, table, ready, gathered, folded, total,
    token_sem, load_sem, own_sem, send_one, recv_one, send_two, recv_two, send_col, recv_col,
):
    row, col = lax.axis_index("row"), lax.axis_index("col")
    rows = packed.shape[1]
    block, width = packed.shape[3], w_in.shape[1]
    size = block // steps
    part = packed.shape[2]
    flip = lambda index, bit: index + bit - 2 * bit * (index // bit % 2)
    sibling, across = flip(col, 1), flip(col, 2)

    def mate(d):
        index = row
        for bit in (1, 2, 4):
            if d & bit:
                index = flip(index, bit)
        return index

    loads = [
        pltpu.make_async_copy(src, dst, load_sem.at[i])
        for i, (src, dst) in enumerate([
            (w_in_hbm, w_in), (gain_hbm, gain), (forward_hbm, forward), (coarse_hbm, coarse), (fine_hbm, fine),
            (twiddle_hbm, twiddles), (fold_hbm, fold), (w_out_hbm, w_out),
        ])
    ]
    token_loads = [
        pltpu.make_async_copy(
            tokens_hbm.at[pl.ds(p * size, size)], tokens.at[pl.ds(p * size, size)], token_sem.at[p]
        )
        for p in range(steps)
    ]
    for load in loads[:3] + token_loads[:ahead]:
        load.start()

    barrier = pltpu.get_barrier_semaphore()
    peers = [(mate(d), col) for d in range(1, rows)] + [(row, sibling), (row, across)]
    for peer in peers:
        pl.semaphore_signal(barrier, inc=1, device_id=peer, device_id_type=MESH)

    def remote(src, dst, send, recv, device):
        return pltpu.make_async_remote_copy(
            src_ref=src, dst_ref=dst, send_sem=send, recv_sem=recv, device_id=device, device_id_type=MESH
        )

    def first_send(h, d, p=None):
        peer = mate(d)
        where = pl.ds(0, block) if p is None else pl.ds(p * size, size)
        return remote(
            packed.at[h, peer, :, where], arrived.at[h, row, :, where],
            send_one.at[h, d], recv_one.at[h, d], (peer, col),
        )

    order = [4, 5, 6, 7, 2, 3, 1]
    for load in loads[:3]:
        load.wait()
    for p in range(steps):
        token_loads[p].wait()
        if p + ahead < steps:
            token_loads[p + ahead].start()
        elif p + ahead == steps:
            for load in loads[3:]:
                load.start()
        where = slice(p * size, (p + 1) * size)
        wide = tokens[where, :].astype(jnp.float32)
        inverse = lax.rsqrt(jnp.mean(wide * wide, axis=1, keepdims=True) + NORM_EPS)
        normed = (wide * inverse * gain[...]).astype(jnp.bfloat16)
        projected = jnp.dot(normed, w_in[...], preferred_element_type=jnp.float32).astype(jnp.bfloat16)
        kept = lax.dot_general(
            forward[...], projected, (((1,), (1,)), ((), ())), preferred_element_type=jnp.float32
        )
        packed[:, :, :, where] = kept.astype(jnp.bfloat16).reshape(HALVES, rows, part, size)
        if p == 0:
            pl.semaphore_wait(barrier, len(peers))
        for d in order:
            first_send(0, d, p).start()
    for d in order:
        first_send(1, d).start()
    own_one = [
        pltpu.make_async_copy(packed.at[h, row], arrived.at[h, row], own_sem.at[h]) for h in range(HALVES)
    ]
    for copy in own_one:
        copy.start()
    for load in loads[3:]:
        load.wait()

    root = fine.shape[1]

    def table_rows(a, carry):
        cos_a, sin_a = coarse[0, pl.ds(a, 1), :], coarse[1, pl.ds(a, 1), :]
        at = pl.multiple_of(a * root, root)
        table[pl.ds(at, root), :] = (cos_a * fine[0] - sin_a * fine[1]).astype(jnp.bfloat16)
        table[pl.ds(block + at, root), :] = (sin_a * fine[0] + cos_a * fine[1]).astype(jnp.bfloat16)
        return carry

    lax.fori_loop(0, block // root, table_rows, 0)
    cols = w_out.shape[0] // width
    half = width // HALVES
    for c in range(cols):
        rows_out = jnp.dot(
            fold[...], w_out[c * width : (c + 1) * width, :], preferred_element_type=jnp.float32
        ).astype(jnp.bfloat16)
        for h in range(HALVES):
            folded[h, c * half : (c + 1) * half, :] = rows_out[h * half : (h + 1) * half]

    cut = POINTS // SPLIT

    def second_send(g, d):
        h, where = g // SPLIT, pl.ds(g % SPLIT * cut, cut)
        peer = mate(d)
        return remote(
            ready.at[h, peer, where], gathered.at[h, col, row, where],
            send_two.at[g, d], recv_two.at[g, d], (peer, col),
        )

    def keep(g):
        h, where = g // SPLIT, pl.ds(g % SPLIT * cut, cut)
        return pltpu.make_async_copy(
            ready.at[h, row, where], gathered.at[h, col, row, where], own_sem.at[HALVES + g]
        )

    span = 2 * LANES
    count = block // span
    other = (1 - row // (rows // 2)) * (count // 2)
    far, close = order[: rows // 2], order[rows // 2 :]
    for h in range(HALVES):
        own_one[h].wait()
        for d in order:
            first_send(h, d).wait_recv()

        def section(t, carry):
            at = pl.multiple_of(t * LANES, LANES)
            x = [arrived[h, r, :, pl.ds(at, LANES)].astype(jnp.float32) for r in range(rows)]
            points = eight_points(x)
            for k in range(POINTS):
                real, imag = points[k]
                if k > 0:
                    cosine = twiddles[0, k : k + 1, pl.ds(at, LANES)]
                    sine = twiddles[1, k : k + 1, pl.ds(at, LANES)]
                    if imag is None:
                        real, imag = real * cosine, -real * sine
                    else:
                        real, imag = real * cosine + imag * sine, imag * cosine - real * sine
                else:
                    imag = jnp.zeros_like(real)
                if h == 1:
                    place = lax.broadcasted_iota(jnp.int32, real.shape, 0) + row * part
                    plain = place == 0
                    real, imag = jnp.where(plain, real, -imag), jnp.where(plain, imag, real)
                stage[k, :, pl.ds(at, LANES)] = real.astype(jnp.bfloat16)
                stage[k, :, pl.ds(pl.multiple_of(block + at, LANES), LANES)] = imag.astype(jnp.bfloat16)
            return carry

        lax.fori_loop(0, block // LANES, section, 0)
        values = stage[...].reshape(POINTS * part, 2 * block)
        for i in range(count):
            n = lax.rem(other + i, count)
            done = jnp.dot(
                values, table[:, pl.ds(pl.multiple_of(n * span, span), span)], preferred_element_type=jnp.float32
            ).astype(jnp.bfloat16)
            for q in range(2):
                ready[h, 2 * n + q] = done[:, q * LANES : (q + 1) * LANES].reshape(POINTS, part, LANES)
            if i == count // 2 - 1:
                for g in range(h * SPLIT, (h + 1) * SPLIT):
                    for d in far:
                        second_send(g, d).start()
        for g in range(h * SPLIT, (h + 1) * SPLIT):
            for d in close:
                second_send(g, d).start()
            keep(g).start()

    def along(g, way, owner, target, d):
        spot = gathered.at[g // SPLIT, owner, mate(d), pl.ds(g % SPLIT * cut, cut)]
        return remote(spot, spot, send_col.at[g, way, d], recv_col.at[g, way, d], (row, target))

    def to_across(g, d):
        return along(g, 0, col, across, d)

    def to_sibling(g, d):
        return along(g, 1, col, sibling, d)

    def on_to_sibling(g, d):
        return along(g, 2, across, sibling, d)

    near, every = [0] + close[::-1], [0] + close[::-1] + far

    def relay(g, origins):
        for d in origins:
            if d == 0:
                keep(g).wait()
            else:
                second_send(g, d).wait_recv()
            to_across(g, d).start()
            to_sibling(g, d).start()

    def pass_on(g, origins):
        for d in origins:
            to_across(g, d).wait_recv()
            on_to_sibling(g, d).start()

    def collect(g):
        for d in every:
            to_sibling(g, d).wait_recv()
            on_to_sibling(g, d).wait_recv()

    def map_out(h, k):
        spectrum = gathered[h, :, :, k].reshape(cols * rows * part, LANES)
        piece = lax.dot_general(
            spectrum, folded[h], (((0,), (0,)), ((), ())), preferred_element_type=jnp.float32
        )
        total[k] = piece if h == 0 else total[k] + piece

    def map_part(g):
        for k in range(g % SPLIT * cut, (g % SPLIT + 1) * cut):
            map_out(g // SPLIT, k)

    relay(0, every)
    for d in every:
        relay(1, [d])
        pass_on(0, [d])
    collect(0)
    for k, d in enumerate(every):
        map_out(0, k)
        pass_on(1, [d])
    collect(1)
    map_part(1)
    out_ref[...] = jnp.swapaxes(total[...], 0, 1).reshape(out_ref.shape).astype(out_ref.dtype)

    for h in range(HALVES):
        for d in order:
            first_send(h, d).wait_send()
    for g in range(HALVES * SPLIT):
        for d in order:
            second_send(g, d).wait_send()
        for d in every:
            to_across(g, d).wait_send()
            to_sibling(g, d).wait_send()
            on_to_sibling(g, d).wait_send()


def fused(tokens, norm_gain, w_in, w_out):
    rows, cols = lax.axis_size("row"), lax.axis_size("col")
    block, width_in = tokens.shape
    width = w_in.shape[1]
    features = w_out.shape[1]
    part = width // (HALVES * rows)
    steps = 4
    forward, fold = channel_tables(width, block * rows)
    twiddles, coarse, fine = position_tables(block, block * rows)
    half, short, wide = jnp.bfloat16, pltpu.VMEM, jnp.float32
    operands = [tokens, norm_gain[None, :], w_in, w_out, forward, fold, twiddles, coarse, fine]
    operands = [pltpu.with_memory_space_constraint(jnp.asarray(x), pltpu.HBM) for x in operands]
    dma = pltpu.SemaphoreType.DMA
    return pl.pallas_call(
        functools.partial(mixer_kernel, steps, 2),
        out_shape=jax.ShapeDtypeStruct((block, features), half),
        in_specs=[pl.BlockSpec(memory_space=pl.ANY)] * len(operands),
        out_specs=pl.BlockSpec(memory_space=pltpu.VMEM),
        scratch_shapes=[short(x.shape, x.dtype) for x in operands]
        + [
            short((HALVES, rows, part, block), half),
            short((HALVES, rows, part, block), half),
            short((POINTS, part, 2 * block), half),
            short((2 * block, block), half),
            short((HALVES, rows, POINTS, part, LANES), half),
            short((HALVES, cols, rows, POINTS, part, LANES), half),
            short((HALVES, w_out.shape[0] // HALVES, features), half),
            short((POINTS, LANES, features), wide),
            dma((steps,)),
            dma((8,)),
            dma((HALVES + HALVES * SPLIT,)),
            dma((HALVES, rows)),
            dma((HALVES, rows)),
            dma((HALVES * SPLIT, rows)),
            dma((HALVES * SPLIT, rows)),
            dma((HALVES * SPLIT, 3, rows)),
            dma((HALVES * SPLIT, 3, rows)),
        ],
        compiler_params=pltpu.CompilerParams(
            collective_id=0, has_side_effects=True, vmem_limit_bytes=32 * 1024 * 1024
        ),
    )(*operands)


def fits(mesh):
    return mesh.shape["row"] == POINTS and mesh.shape["col"] == 4


def choose(mesh, *arrays):
    tokens, _, w_in, _ = arrays
    group_local = w_in.shape[1] == GROUP
    tiles = tokens.shape[0] == POINTS * LANES
    return fused(*arrays) if fits(mesh) and group_local and tiles else local(*arrays)


def solution(mesh):
    placed = (P("row", None), P(), P(None, "col"), P(None, "col"))
    return jax.shard_map(
        functools.partial(choose, mesh), mesh=mesh, in_specs=placed, out_specs=P("row", "col"), check_vma=False
    )
```

```python
import functools
import math

import jax
import jax.numpy as jnp
import numpy as np
from jax import lax
from jax.experimental import pallas as pl
from jax.experimental.pallas import tpu as pltpu
from jax.sharding import PartitionSpec as P

GROUP = 256


NORM_EPS = 1e-06


def as_sent(array):

    def short(part):
        return part.astype(jnp.bfloat16) if part.dtype == jnp.float32 else part

    return jax.tree.map(short, array)


def rotation_table(first_index, second_index, spectral_magnitude, factor):
    phase = (first_index * second_index % spectral_magnitude).astype(jnp.float32) * (
        2.0 * math.pi / spectral_magnitude
    )
    return (jnp.cos(phase) * factor, jnp.sin(phase) * factor)


def twiddle(real_input_values, imag_in, freq_index, pos_index, spectral_magnitude):
    cosine, sine = rotation_table(freq_index, pos_index, spectral_magnitude, 1.0)
    return (
        real_input_values * cosine + imag_in * sine,
        imag_in * cosine - real_input_values * sine,
    )


def second_section(stacked, half):
    length_dev = stacked.shape[1]
    stride = min(length_dev, 512)
    positions = lax.broadcasted_iota(jnp.int32, (length_dev, stride), 0)
    real_blocks = []
    imag_blocks = []
    for offset in range(0, length_dev, stride):
        freqs = lax.broadcasted_iota(jnp.int32, (length_dev, stride), 1) + offset
        cosine, sine = rotation_table(positions, freqs, length_dev, 1.0)
        with_cos = jnp.dot(stacked, cosine, precision=lax.Precision.HIGH)
        with_sin = jnp.dot(stacked, sine, precision=lax.Precision.HIGH)
        real_blocks.append(with_cos[:half] + with_sin[half:])
        imag_blocks.append(with_cos[half:] - with_sin[:half])
    return (jnp.concatenate(real_blocks, 1), jnp.concatenate(imag_blocks, 1))


def reorder_positions(arrived):
    channels, row_count, _, block_len = arrived.shape
    return jnp.swapaxes(arrived.reshape(channels, row_count, block_len), 1, 2).reshape(
        channels, row_count * block_len
    )


def local(tokens, norm_gain, w_in, w_out):
    length_dev = tokens.shape[0]
    row_count = lax.axis_size("row")
    col_count = lax.axis_size("col")
    total_len = length_dev * row_count
    widened = tokens.astype(jnp.float32)
    inverse = lax.rsqrt(jnp.mean(widened * widened, axis=1, keepdims=True) + NORM_EPS)
    normed = (widened * inverse * norm_gain[None, :]).astype(jnp.bfloat16)
    projected = lax.dot_general(
        w_in, normed, (((0,), (1,)), ((), ())), preferred_element_type=jnp.float32
    ).astype(jnp.bfloat16)
    channels = projected.shape[0]
    block_len = length_dev // row_count
    small_cos, small_sin = rotation_table(
        lax.broadcasted_iota(jnp.int32, (row_count, row_count), 0),
        lax.broadcasted_iota(jnp.int32, (row_count, row_count), 1),
        row_count,
        1.0 / math.sqrt(total_len),
    )
    per_row = channels // row_count
    arrived = lax.all_to_all(
        projected.reshape(channels, 1, length_dev), "row", split_axis=0, concat_axis=1, tiled=True
    )
    values = arrived.astype(jnp.float32)
    real_one = jnp.einsum("ka,cab->ckb", small_cos, values, precision=lax.Precision.HIGH)
    imag_one = -jnp.einsum("ka,cab->ckb", small_sin, values, precision=lax.Precision.HIGH)
    freq_index = lax.broadcasted_iota(jnp.int32, (row_count, length_dev), 0)
    pos_index = lax.broadcasted_iota(jnp.int32, (row_count, length_dev), 1)
    real_two, imag_two = twiddle(real_one, imag_one, freq_index, pos_index, total_len)
    stacked = jnp.concatenate(
        [
            real_two.reshape(per_row * row_count, length_dev),
            imag_two.reshape(per_row * row_count, length_dev),
        ],
        0,
    )
    real_three, imag_three = second_section(stacked, per_row * row_count)
    shaped = (per_row, row_count, row_count, block_len)
    back_real, back_imag = (
        lax.all_to_all(
            real_three.reshape(shaped).astype(jnp.bfloat16),
            "row",
            split_axis=2,
            concat_axis=0,
            tiled=True,
        ).astype(jnp.float32),
        lax.all_to_all(
            imag_three.reshape(shaped).astype(jnp.bfloat16),
            "row",
            split_axis=2,
            concat_axis=0,
            tiled=True,
        ).astype(jnp.float32),
    )
    spec_real = reorder_positions(back_real)
    spec_imag = reorder_positions(back_imag)
    quarter = length_dev // col_count
    group_cosine_table, group_sine_table = rotation_table(
        lax.broadcasted_iota(jnp.int32, (GROUP, GROUP), 0),
        lax.broadcasted_iota(jnp.int32, (GROUP, GROUP), 1),
        GROUP,
        1.0 / math.sqrt(GROUP),
    )
    real_input_values = lax.all_to_all(
        as_sent(spec_real.reshape(channels, col_count, quarter)),
        "col",
        split_axis=1,
        concat_axis=0,
        tiled=True,
    )
    imag_in = lax.all_to_all(
        as_sent(spec_imag.reshape(channels, col_count, quarter)),
        "col",
        split_axis=1,
        concat_axis=0,
        tiled=True,
    )
    width_all = real_input_values.shape[0]
    item_count = real_input_values.shape[2]
    groups = width_all // GROUP
    real_by_group = real_input_values.reshape(groups, GROUP, item_count)
    imaginary_by_group = imag_in.reshape(groups, GROUP, item_count)
    merged_spectrum = jnp.einsum(
        "hz,azo->aho", group_cosine_table, real_by_group, precision=lax.Precision.HIGH
    )
    merged_spectrum = merged_spectrum + jnp.einsum(
        "hz,azo->aho", group_sine_table, imaginary_by_group, precision=lax.Precision.HIGH
    )
    result = merged_spectrum.reshape(width_all, 1, item_count).astype(jnp.bfloat16)
    spectral = lax.all_to_all(result, "col", split_axis=0, concat_axis=1, tiled=True)
    output = lax.dot_general(
        lax.all_gather(spectral.reshape(channels, length_dev), "col", axis=0, tiled=True),
        w_out,
        (((0,), (0,)), ((), ())),
        preferred_element_type=jnp.float32,
    )
    return output.astype(jnp.bfloat16)


HALVES = 2
POINTS = 8
LANES = 128
MESH = pl.DeviceIdType.MESH


def channel_tables(group, total_len):
    half = group // 2
    index = np.arange(group)
    angle = 2.0 * np.pi * (index[:, None] * index[None, :] % group) / group
    transform = np.concatenate([np.cos(angle[: half + 1]), np.sin(angle[1:half])], 0)
    fold = np.zeros((group, group))
    for k in range(half + 1):
        fold[k, k] = 1.0
        fold[k, -k % group] = 1.0
    for k in range(1, half):
        fold[half + k, group - k] = 1.0
        fold[half + k, k] = -1.0
    return (transform / math.sqrt(group)).astype(jnp.bfloat16), fold.astype(jnp.bfloat16)


def position_tables(block, total_len):
    j = np.arange(block)
    angle = 2.0 * np.pi * (np.arange(POINTS)[:, None] * j[None, :]) / total_len
    twiddles = np.stack([np.cos(angle), np.sin(angle)]).astype(np.float32)
    root = 32
    coarse = 2.0 * np.pi * (np.arange(block // root)[:, None] * root * j[None, :] % block) / block
    fine = 2.0 * np.pi * (np.arange(root)[:, None] * j[None, :] % block) / block
    scale = 1.0 / math.sqrt(total_len)
    coarse = np.stack([np.cos(coarse), np.sin(coarse)]).astype(np.float32)
    fine = np.stack([np.cos(fine) * scale, np.sin(fine) * scale]).astype(np.float32)
    return twiddles, coarse, fine


def eight_points(x):
    a = [x[i] + x[i + 4] for i in range(4)]
    b = [x[i] - x[i + 4] for i in range(4)]
    even, odd = a[0] + a[2], a[1] + a[3]
    root = math.sqrt(0.5)
    minus, plus = root * (b[1] - b[3]), root * (b[1] + b[3])
    one = (b[0] + minus, -b[2] - plus)
    two = (a[0] - a[2], a[3] - a[1])
    three = (b[0] - minus, b[2] - plus)
    return [
        (even + odd, None),
        one,
        two,
        three,
        (even - odd, None),
        (three[0], -three[1]),
        (two[0], -two[1]),
        (one[0], -one[1]),
    ]


def mixer_kernel(
    steps, ahead, direct,
    tokens_hbm, gain_hbm, w_in_hbm, w_out_hbm, forward_hbm, fold_hbm, twiddle_hbm, coarse_hbm, fine_hbm,
    out_ref,
    tokens, gain, w_in, w_out, forward, fold, twiddles, coarse, fine,
    packed, arrived, stage, table, ready, gathered, folded, total,
    token_sem, load_sem, send_one, recv_one, send_two, recv_near, recv_far, recv_direct, recv_relay, recv_share,
):
    row, col = lax.axis_index("row"), lax.axis_index("col")
    rows = packed.shape[1]
    block, width = packed.shape[3], w_in.shape[1]
    size = block // steps
    part = packed.shape[2]
    flip = lambda index, bit: index + bit - 2 * bit * (index // bit % 2)
    sibling, across = flip(col, 1), flip(col, 2)
    quarter = rows // 2
    near, far = list(range(quarter)), list(range(quarter, rows))

    def mate(d):
        index = row
        for bit in (1, 2, 4):
            if d & bit:
                index = flip(index, bit)
        return index

    loads = [
        pltpu.make_async_copy(src, dst, load_sem.at[i])
        for i, (src, dst) in enumerate([
            (w_in_hbm, w_in), (gain_hbm, gain), (forward_hbm, forward), (coarse_hbm, coarse), (fine_hbm, fine),
            (twiddle_hbm, twiddles), (fold_hbm, fold), (w_out_hbm, w_out),
        ])
    ]
    token_loads = [
        pltpu.make_async_copy(
            tokens_hbm.at[pl.ds(p * size, size)], tokens.at[pl.ds(p * size, size)], token_sem.at[p]
        )
        for p in range(steps)
    ]
    for load in loads[:3] + token_loads[:ahead]:
        load.start()

    barrier = pltpu.get_barrier_semaphore()
    peers = [(mate(d), col) for d in range(1, rows)] + [(row, sibling)]
    peers += [(mate(d), across) for d in range(rows) if d == 0 or d in direct]
    for peer in peers:
        pl.semaphore_signal(barrier, inc=1, device_id=peer, device_id_type=MESH)

    def remote(src, dst, send, recv, device):
        return pltpu.make_async_remote_copy(
            src_ref=src, dst_ref=dst, send_sem=send, recv_sem=recv, device_id=device, device_id_type=MESH
        )

    def first_send(h, d, where):
        peer = mate(d)
        return remote(
            packed.at[h, peer, :, where], arrived.at[h, row, :, where], send_one, recv_one.at[h], (peer, col)
        )

    order = far + [2, 3, 1]
    for load in loads[:3]:
        load.wait()
    for p in range(steps):
        token_loads[p].wait()
        if p + ahead < steps:
            token_loads[p + ahead].start()
        elif p + ahead == steps:
            for load in loads[3:]:
                load.start()
        where = slice(p * size, (p + 1) * size)
        wide = tokens[where, :].astype(jnp.float32)
        inverse = lax.rsqrt(jnp.mean(wide * wide, axis=1, keepdims=True) + NORM_EPS)
        normed = (wide * inverse * gain[...]).astype(jnp.bfloat16)
        projected = jnp.dot(normed, w_in[...], preferred_element_type=jnp.float32).astype(jnp.bfloat16)
        kept = lax.dot_general(
            forward[...], projected, (((1,), (1,)), ((), ())), preferred_element_type=jnp.float32
        )
        packed[:, :, :, where] = kept.astype(jnp.bfloat16).reshape(HALVES, rows, part, size)
        if p == 0:
            pl.semaphore_wait(barrier, len(peers))
        for d in order:
            first_send(0, d, pl.ds(p * size, size)).start()
    for d in order:
        first_send(1, d, pl.ds(0, block)).start()
    for h in range(HALVES):
        arrived[h, row] = packed[h, row]
    for load in loads[3:]:
        load.wait()

    root = fine.shape[1]

    def table_rows(a, carry):
        cos_a, sin_a = coarse[0, pl.ds(a, 1), :], coarse[1, pl.ds(a, 1), :]
        at = pl.multiple_of(a * root, root)
        table[pl.ds(at, root), :] = (cos_a * fine[0] - sin_a * fine[1]).astype(jnp.bfloat16)
        table[pl.ds(block + at, root), :] = (sin_a * fine[0] + cos_a * fine[1]).astype(jnp.bfloat16)
        return carry

    lax.fori_loop(0, block // root, table_rows, 0)
    cols = w_out.shape[0] // width
    half = width // HALVES
    for c in range(cols):
        rows_out = jnp.dot(
            fold[...], w_out[c * width : (c + 1) * width, :], preferred_element_type=jnp.float32
        ).astype(jnp.bfloat16)
        for h in range(HALVES):
            folded[h, c] = rows_out[h * half : (h + 1) * half].reshape(rows, part, -1)

    pieces = gathered.at[0, 0]
    send_far, send_near, send_direct, send_relay, send_share = (send_two.at[i] for i in range(5))

    def second_send(h, d):
        peer = mate(d)
        recv = recv_far.at[h, d - quarter] if d in far else recv_near.at[h]
        return remote(
            ready.at[h, peer], gathered.at[h, col, row], send_far if d in far else send_near, recv, (peer, col)
        )

    def direct_send(h, d):
        peer = mate(d)
        return remote(
            ready.at[h, peer], gathered.at[h, col, row], send_direct, recv_direct.at[h], (peer, across)
        )

    def relay_send(h, d):
        spot = gathered.at[h, col, mate(d)]
        recv = recv_relay.at[h, d // 2]
        return remote(spot, spot, send_relay, recv, (row, across))

    def share(h, owner, start, count, kind):
        spot = gathered.at[h, owner, pl.ds(start, count)]
        return remote(spot, spot, send_share, recv_share.at[h, kind], (row, sibling))

    def waiter(count, send, recv):
        group = pieces.at[pl.ds(0, count)]
        return remote(group, group, send, recv, (row, sibling))

    span = 2 * LANES
    for h in range(HALVES):
        others = pl.ds(0, rows - 1)
        remote(
            packed.at[h, others], arrived.at[h, others], send_one, recv_one.at[h], (row, sibling)
        ).wait_recv()

        def section(t, carry):
            at = pl.multiple_of(t * LANES, LANES)
            x = [arrived[h, r, :, pl.ds(at, LANES)].astype(jnp.float32) for r in range(rows)]
            points = eight_points(x)
            for k in range(POINTS):
                real, imag = points[k]
                if k > 0:
                    cosine = twiddles[0, k : k + 1, pl.ds(at, LANES)]
                    sine = twiddles[1, k : k + 1, pl.ds(at, LANES)]
                    if imag is None:
                        real, imag = real * cosine, -real * sine
                    else:
                        real, imag = real * cosine + imag * sine, imag * cosine - real * sine
                else:
                    imag = jnp.zeros_like(real)
                if h == 1:
                    place = lax.broadcasted_iota(jnp.int32, real.shape, 0) + row * part
                    plain = place == 0
                    real, imag = jnp.where(plain, real, -imag), jnp.where(plain, imag, real)
                stage[k, :, pl.ds(at, LANES)] = real.astype(jnp.bfloat16)
                stage[k, :, pl.ds(pl.multiple_of(block + at, LANES), LANES)] = imag.astype(jnp.bfloat16)
            return carry

        lax.fori_loop(0, block // LANES, section, 0)
        values = stage[...].reshape(POINTS * part, 2 * block)
        for base in (4, 6, 2, 0):
            n = mate(base) // 2
            done = jnp.dot(
                values, table[:, pl.ds(pl.multiple_of(n * span, span), span)], preferred_element_type=jnp.float32
            ).astype(jnp.bfloat16)
            for q in range(2):
                ready[h, 2 * n + q] = done[:, q * LANES : (q + 1) * LANES].reshape(POINTS, part, LANES)
            for d in (base, base + 1):
                if d > 0:
                    second_send(h, d).start()
                if d in direct:
                    direct_send(h, d).start()
        gathered[h, col, row] = ready[h, row]

    base_near = row // quarter * quarter
    base_far = quarter - base_near
    pairs = [quarter // 2 + i for i in range(quarter // 2)]
    pair_row = lambda pair: mate(2 * pair) // 2 * 2

    def relay(h, d):
        second_send(h, d).wait_recv()
        relay_send(h, d).start()
        if d % 2 == 1:
            share(h, col, pair_row(d // 2), 2, 1).start()

    def pass_on(h, pair):
        waiter(2, send_relay, recv_relay.at[h, pair]).wait_recv()
        share(h, across, pair_row(pair), 2, 1).start()

    def share_near(h):
        waiter(quarter - 1, send_near, recv_near.at[h]).wait_recv()
        share(h, col, base_near, quarter, 0).start()
        waiter(quarter, send_direct, recv_direct.at[h]).wait_recv()
        share(h, across, base_near, quarter, 0).start()

    def collect(h, kind):
        waiter(rows, send_share, recv_share.at[h, kind]).wait_recv()

    depth = cols * quarter * part

    def map_out(h, kind, k):
        start = base_far if kind else base_near
        spectrum = gathered[h, :, pl.ds(start, quarter), k].reshape(depth, LANES)
        weights = folded[h, :, pl.ds(start, quarter)].reshape(depth, -1)
        piece = lax.dot_general(
            spectrum, weights, (((0,), (0,)), ((), ())), preferred_element_type=jnp.float32
        )
        total[k] = piece if h == 0 and kind == 0 else total[k] + piece

    def map_part(h, kind):
        for k in range(POINTS):
            map_out(h, kind, k)

    for d in far:
        relay(0, d)
    share_near(0)
    relay(1, far[0])
    collect(0, 0)
    map_part(0, 0)
    for pair in pairs:
        pass_on(0, pair)
    for d in far[1:]:
        relay(1, d)
    share_near(1)
    collect(0, 1)
    map_part(0, 1)
    collect(1, 0)
    map_part(1, 0)
    for pair in pairs:
        pass_on(1, pair)
    collect(1, 1)
    map_part(1, 1)
    out_ref[...] = jnp.swapaxes(total[...], 0, 1).reshape(out_ref.shape).astype(out_ref.dtype)

    others = pl.ds(0, rows - 1)
    remote(packed.at[:, others], arrived.at[:, others], send_one, recv_one.at[0], (row, sibling)).wait_send()
    waiter(HALVES * len(far), send_far, recv_far.at[0, 0]).wait_send()
    waiter(HALVES * (quarter - 1), send_near, recv_near.at[0]).wait_send()
    waiter(HALVES * len(direct), send_direct, recv_direct.at[0]).wait_send()
    waiter(HALVES * len(far), send_relay, recv_relay.at[0, 0]).wait_send()
    everything = gathered.at[0]
    remote(everything, everything, send_share, recv_share.at[0, 0], (row, sibling)).wait_send()


def fused(tokens, norm_gain, w_in, w_out):
    rows, cols = lax.axis_size("row"), lax.axis_size("col")
    block, width_in = tokens.shape
    width = w_in.shape[1]
    features = w_out.shape[1]
    part = width // (HALVES * rows)
    steps = 4
    forward, fold = channel_tables(width, block * rows)
    twiddles, coarse, fine = position_tables(block, block * rows)
    half, short, wide = jnp.bfloat16, pltpu.VMEM, jnp.float32
    operands = [tokens, norm_gain[None, :], w_in, w_out, forward, fold, twiddles, coarse, fine]
    operands = [pltpu.with_memory_space_constraint(jnp.asarray(x), pltpu.HBM) for x in operands]
    dma = pltpu.SemaphoreType.DMA
    direct = (0, 1, 2, 3)
    return pl.pallas_call(
        functools.partial(mixer_kernel, steps, 2, direct),
        out_shape=jax.ShapeDtypeStruct((block, features), half),
        in_specs=[pl.BlockSpec(memory_space=pl.ANY)] * len(operands),
        out_specs=pl.BlockSpec(memory_space=pltpu.VMEM),
        scratch_shapes=[short(x.shape, x.dtype) for x in operands]
        + [
            short((HALVES, rows, part, block), half),
            short((HALVES, rows, part, block), half),
            short((POINTS, part, 2 * block), half),
            short((2 * block, block), half),
            short((HALVES, rows, POINTS, part, LANES), half),
            short((HALVES, cols, rows, POINTS, part, LANES), half),
            short((HALVES, cols, rows, part, features), half),
            short((POINTS, LANES, features), wide),
            dma((steps,)),
            dma((8,)),
            dma(()),
            dma((HALVES,)),
            dma((5,)),
            dma((HALVES,)),
            dma((HALVES, rows // 2)),
            dma((HALVES,)),
            dma((HALVES, rows // 2)),
            dma((HALVES, 2)),
        ],
        compiler_params=pltpu.CompilerParams(
            collective_id=0, has_side_effects=True, vmem_limit_bytes=32 * 1024 * 1024
        ),
    )(*operands)


def fits(mesh):
    return mesh.shape["row"] == POINTS and mesh.shape["col"] == 4


def choose(mesh, *arrays):
    tokens, _, w_in, _ = arrays
    group_local = w_in.shape[1] == GROUP
    tiles = tokens.shape[0] == POINTS * LANES
    return fused(*arrays) if fits(mesh) and group_local and tiles else local(*arrays)


def solution(mesh):
    placed = (P("row", None), P(), P(None, "col"), P(None, "col"))
    return jax.shard_map(
        functools.partial(choose, mesh), mesh=mesh, in_specs=placed, out_specs=P("row", "col"), check_vma=False
    )
```

```python
import functools
import math

import jax
import jax.numpy as jnp
import numpy as np
from jax import lax
from jax.experimental import pallas as pl
from jax.experimental.pallas import tpu as pltpu
from jax.sharding import PartitionSpec as P

GROUP = 256


NORM_EPS = 1e-06


def as_sent(array):

    def short(part):
        return part.astype(jnp.bfloat16) if part.dtype == jnp.float32 else part

    return jax.tree.map(short, array)


def rotation_table(first_index, second_index, spectral_magnitude, factor):
    phase = (first_index * second_index % spectral_magnitude).astype(jnp.float32) * (
        2.0 * math.pi / spectral_magnitude
    )
    return (jnp.cos(phase) * factor, jnp.sin(phase) * factor)


def twiddle(real_input_values, imag_in, freq_index, pos_index, spectral_magnitude):
    cosine, sine = rotation_table(freq_index, pos_index, spectral_magnitude, 1.0)
    return (
        real_input_values * cosine + imag_in * sine,
        imag_in * cosine - real_input_values * sine,
    )


def second_section(stacked, half):
    length_dev = stacked.shape[1]
    stride = min(length_dev, 512)
    positions = lax.broadcasted_iota(jnp.int32, (length_dev, stride), 0)
    real_blocks = []
    imag_blocks = []
    for offset in range(0, length_dev, stride):
        freqs = lax.broadcasted_iota(jnp.int32, (length_dev, stride), 1) + offset
        cosine, sine = rotation_table(positions, freqs, length_dev, 1.0)
        with_cos = jnp.dot(stacked, cosine, precision=lax.Precision.HIGH)
        with_sin = jnp.dot(stacked, sine, precision=lax.Precision.HIGH)
        real_blocks.append(with_cos[:half] + with_sin[half:])
        imag_blocks.append(with_cos[half:] - with_sin[:half])
    return (jnp.concatenate(real_blocks, 1), jnp.concatenate(imag_blocks, 1))


def reorder_positions(arrived):
    channels, row_count, _, block_len = arrived.shape
    return jnp.swapaxes(arrived.reshape(channels, row_count, block_len), 1, 2).reshape(
        channels, row_count * block_len
    )


def local(tokens, norm_gain, w_in, w_out):
    length_dev = tokens.shape[0]
    row_count = lax.axis_size("row")
    col_count = lax.axis_size("col")
    total_len = length_dev * row_count
    widened = tokens.astype(jnp.float32)
    inverse = lax.rsqrt(jnp.mean(widened * widened, axis=1, keepdims=True) + NORM_EPS)
    normed = (widened * inverse * norm_gain[None, :]).astype(jnp.bfloat16)
    projected = lax.dot_general(
        w_in, normed, (((0,), (1,)), ((), ())), preferred_element_type=jnp.float32
    ).astype(jnp.bfloat16)
    channels = projected.shape[0]
    block_len = length_dev // row_count
    small_cos, small_sin = rotation_table(
        lax.broadcasted_iota(jnp.int32, (row_count, row_count), 0),
        lax.broadcasted_iota(jnp.int32, (row_count, row_count), 1),
        row_count,
        1.0 / math.sqrt(total_len),
    )
    per_row = channels // row_count
    arrived = lax.all_to_all(
        projected.reshape(channels, 1, length_dev), "row", split_axis=0, concat_axis=1, tiled=True
    )
    values = arrived.astype(jnp.float32)
    real_one = jnp.einsum("ka,cab->ckb", small_cos, values, precision=lax.Precision.HIGH)
    imag_one = -jnp.einsum("ka,cab->ckb", small_sin, values, precision=lax.Precision.HIGH)
    freq_index = lax.broadcasted_iota(jnp.int32, (row_count, length_dev), 0)
    pos_index = lax.broadcasted_iota(jnp.int32, (row_count, length_dev), 1)
    real_two, imag_two = twiddle(real_one, imag_one, freq_index, pos_index, total_len)
    stacked = jnp.concatenate(
        [
            real_two.reshape(per_row * row_count, length_dev),
            imag_two.reshape(per_row * row_count, length_dev),
        ],
        0,
    )
    real_three, imag_three = second_section(stacked, per_row * row_count)
    shaped = (per_row, row_count, row_count, block_len)
    back_real, back_imag = (
        lax.all_to_all(
            real_three.reshape(shaped).astype(jnp.bfloat16),
            "row",
            split_axis=2,
            concat_axis=0,
            tiled=True,
        ).astype(jnp.float32),
        lax.all_to_all(
            imag_three.reshape(shaped).astype(jnp.bfloat16),
            "row",
            split_axis=2,
            concat_axis=0,
            tiled=True,
        ).astype(jnp.float32),
    )
    spec_real = reorder_positions(back_real)
    spec_imag = reorder_positions(back_imag)
    quarter = length_dev // col_count
    group_cosine_table, group_sine_table = rotation_table(
        lax.broadcasted_iota(jnp.int32, (GROUP, GROUP), 0),
        lax.broadcasted_iota(jnp.int32, (GROUP, GROUP), 1),
        GROUP,
        1.0 / math.sqrt(GROUP),
    )
    real_input_values = lax.all_to_all(
        as_sent(spec_real.reshape(channels, col_count, quarter)),
        "col",
        split_axis=1,
        concat_axis=0,
        tiled=True,
    )
    imag_in = lax.all_to_all(
        as_sent(spec_imag.reshape(channels, col_count, quarter)),
        "col",
        split_axis=1,
        concat_axis=0,
        tiled=True,
    )
    width_all = real_input_values.shape[0]
    item_count = real_input_values.shape[2]
    groups = width_all // GROUP
    real_by_group = real_input_values.reshape(groups, GROUP, item_count)
    imaginary_by_group = imag_in.reshape(groups, GROUP, item_count)
    merged_spectrum = jnp.einsum(
        "hz,azo->aho", group_cosine_table, real_by_group, precision=lax.Precision.HIGH
    )
    merged_spectrum = merged_spectrum + jnp.einsum(
        "hz,azo->aho", group_sine_table, imaginary_by_group, precision=lax.Precision.HIGH
    )
    result = merged_spectrum.reshape(width_all, 1, item_count).astype(jnp.bfloat16)
    spectral = lax.all_to_all(result, "col", split_axis=0, concat_axis=1, tiled=True)
    output = lax.dot_general(
        lax.all_gather(spectral.reshape(channels, length_dev), "col", axis=0, tiled=True),
        w_out,
        (((0,), (0,)), ((), ())),
        preferred_element_type=jnp.float32,
    )
    return output.astype(jnp.bfloat16)


HALVES = 2
POINTS = 8
LANES = 128
MESH = pl.DeviceIdType.MESH


def channel_tables(group, total_len):
    half = group // 2
    index = np.arange(group)
    angle = 2.0 * np.pi * (index[:, None] * index[None, :] % group) / group
    transform = np.concatenate([np.cos(angle[: half + 1]), np.sin(angle[1:half])], 0)
    fold = np.zeros((group, group))
    for k in range(half + 1):
        fold[k, k] = 1.0
        fold[k, -k % group] = 1.0
    for k in range(1, half):
        fold[half + k, group - k] = 1.0
        fold[half + k, k] = -1.0
    return (transform / math.sqrt(group)).astype(jnp.bfloat16), fold.astype(jnp.bfloat16)


def position_tables(block, total_len):
    j = np.arange(block)
    angle = 2.0 * np.pi * (np.arange(POINTS)[:, None] * j[None, :]) / total_len
    twiddles = np.stack([np.cos(angle), np.sin(angle)]).astype(np.float32)
    root = 32
    coarse = 2.0 * np.pi * (np.arange(block // root)[:, None] * root * j[None, :] % block) / block
    fine = 2.0 * np.pi * (np.arange(root)[:, None] * j[None, :] % block) / block
    scale = 1.0 / math.sqrt(total_len)
    coarse = np.stack([np.cos(coarse), np.sin(coarse)]).astype(np.float32)
    fine = np.stack([np.cos(fine) * scale, np.sin(fine) * scale]).astype(np.float32)
    return twiddles, coarse, fine


def eight_points(x):
    a = [x[i] + x[i + 4] for i in range(4)]
    b = [x[i] - x[i + 4] for i in range(4)]
    even, odd = a[0] + a[2], a[1] + a[3]
    root = math.sqrt(0.5)
    minus, plus = root * (b[1] - b[3]), root * (b[1] + b[3])
    one = (b[0] + minus, -b[2] - plus)
    two = (a[0] - a[2], a[3] - a[1])
    three = (b[0] - minus, b[2] - plus)
    return [
        (even + odd, None),
        one,
        two,
        three,
        (even - odd, None),
        (three[0], -three[1]),
        (two[0], -two[1]),
        (one[0], -one[1]),
    ]


def mixer_kernel(
    marks, ahead, groups,
    tokens_hbm, gain_hbm, w_in_hbm, w_out_hbm, forward_hbm, fold_hbm, twiddle_hbm, coarse_hbm, fine_hbm,
    out_ref,
    tokens, gain, w_in, w_out, forward, fold, twiddles, coarse, fine,
    packed, arrived, stage, table, ready, gathered, folded, total, spread,
    token_sem, load_sem, send_one, recv_one, send_two, recv_near, recv_far, recv_direct, recv_relay, recv_share,
):
    row, col = lax.axis_index("row"), lax.axis_index("col")
    rows = packed.shape[1]
    block, width = packed.shape[3], w_in.shape[1]
    edges = [block // LANES * LANES * i // 8 for i in marks]
    chunks = [pl.ds(a, b - a) for a, b in zip(edges, edges[1:])]
    steps = len(chunks)
    part = packed.shape[2]
    flip = lambda index, bit: index + bit - 2 * bit * (index // bit % 2)
    sibling, across = flip(col, 1), flip(col, 2)
    quarter = rows // 2
    near, far = list(range(quarter)), list(range(quarter, rows))

    def mate(d):
        index = row
        for bit in (1, 2, 4):
            if d & bit:
                index = flip(index, bit)
        return index

    loads = [
        pltpu.make_async_copy(src, dst, load_sem.at[i])
        for i, (src, dst) in enumerate([
            (w_in_hbm, w_in), (gain_hbm, gain), (forward_hbm, forward), (coarse_hbm, coarse), (fine_hbm, fine),
            (twiddle_hbm, twiddles), (fold_hbm, fold), (w_out_hbm, w_out),
        ])
    ]
    token_loads = [
        pltpu.make_async_copy(tokens_hbm.at[where], tokens.at[where], token_sem.at[p])
        for p, where in enumerate(chunks)
    ]
    for load in [loads[1], loads[0], token_loads[0], loads[2]] + token_loads[1:ahead]:
        load.start()

    barrier = pltpu.get_barrier_semaphore()
    peers = [(mate(d), col) for d in range(1, rows)] + [(row, sibling)]
    peers += [(mate(d), across) for d in near]
    for peer in peers:
        pl.semaphore_signal(barrier, inc=1, device_id=peer, device_id_type=MESH)

    def remote(src, dst, send, recv, device):
        return pltpu.make_async_remote_copy(
            src_ref=src, dst_ref=dst, send_sem=send, recv_sem=recv, device_id=device, device_id_type=MESH
        )

    def first_send(h, d, where):
        peer = mate(d)
        return remote(
            packed.at[h, peer, :, where], arrived.at[h, row, :, where], send_one, recv_one.at[h], (peer, col)
        )

    order = far + [2, 3, 1]
    edge = row // 2 % 3 == 0
    loads[1].wait()
    across_lanes = [
        jnp.transpose(jnp.broadcast_to(gain[:, i : i + LANES], (LANES, LANES)))
        for i in range(0, gain.shape[1], LANES)
    ]
    for i, scale in enumerate(across_lanes):
        spread[i * LANES : (i + 1) * LANES, :] = scale
    loads[0].wait()
    for i in range(0, width, LANES):
        lanes = slice(i, i + LANES)
        w_in[:, lanes] = (w_in[:, lanes].astype(jnp.float32) * spread[...]).astype(jnp.bfloat16)
    loads[2].wait()
    for p, where in enumerate(chunks):
        token_loads[p].wait()
        if p + ahead < steps:
            token_loads[p + ahead].start()
        elif p + ahead == steps:
            for load in loads[3:]:
                load.start()
        piece = tokens[where, :]
        wide = piece.astype(jnp.float32)
        inverse = lax.rsqrt(jnp.mean(wide * wide, axis=1, keepdims=True) + NORM_EPS)
        projected = jnp.dot(piece, w_in[...], preferred_element_type=jnp.float32)
        projected = (projected * inverse).astype(jnp.bfloat16)
        kept = lax.dot_general(
            forward[...], projected, (((1,), (1,)), ((), ())), preferred_element_type=jnp.float32
        )
        packed[:, :, :, where] = kept.astype(jnp.bfloat16).reshape(HALVES, rows, part, where.size)
        if p == 0:
            pl.semaphore_wait(barrier, len(peers))
        for d in order:
            first_send(0, d, where).start()
    def second_half():
        for d in order:
            first_send(1, d, pl.ds(0, block)).start()

    second_half()
    for h in range(HALVES):
        arrived[h, row] = packed[h, row]
    for load in loads[3:]:
        load.wait()

    root = fine.shape[1]

    def table_rows(a, carry):
        cos_a, sin_a = coarse[0, pl.ds(a, 1), :], coarse[1, pl.ds(a, 1), :]
        at = pl.multiple_of(a * root, root)
        table[pl.ds(at, root), :] = (cos_a * fine[0] - sin_a * fine[1]).astype(jnp.bfloat16)
        table[pl.ds(block + at, root), :] = (sin_a * fine[0] + cos_a * fine[1]).astype(jnp.bfloat16)
        return carry

    lax.fori_loop(0, block // root, table_rows, 0)
    cols = w_out.shape[0] // width
    half = width // HALVES
    for c in range(cols):
        rows_out = jnp.dot(
            fold[...], w_out[c * width : (c + 1) * width, :], preferred_element_type=jnp.float32
        ).astype(jnp.bfloat16)
        for h in range(HALVES):
            folded[h, c] = rows_out[h * half : (h + 1) * half].reshape(rows, part, -1)

    base_near = row // quarter * quarter
    base_far = quarter - base_near
    outer = base_far // quarter
    pieces = gathered.at[0, 0]
    send_far, send_near, send_direct, send_relay, send_share = (send_two.at[i] for i in range(5))

    def near_send(h, d):
        return remote(ready.at[h, mate(d)], gathered.at[h, col, row], send_near, recv_near.at[h], (mate(d), col))

    def direct_send(h, d):
        return remote(
            ready.at[h, mate(d)], gathered.at[h, col, row], send_direct, recv_direct.at[h], (mate(d), across)
        )

    def spot(g, owner, place):
        h, first, count = groups[g]
        return gathered.at[h, owner, place, pl.ds(first, count)]

    def crossing(level, f):
        return base_far + 2 * level + flip(row % 2, f)

    def far_send(g, level, f):
        h, first, count = groups[g]
        peer = crossing(level, f)
        return remote(
            ready.at[h, peer, pl.ds(first, count)], spot(g, col, row),
            send_far, recv_far.at[g, row % quarter], (peer, col),
        )

    def far_arrival(g, level, f):
        source = crossing(level, f)
        place = spot(g, col, source)
        return remote(place, place, send_far, recv_far.at[g, source % quarter], (source, col))

    def relay_send(g, level, f):
        place = spot(g, col, crossing(level, f))
        return remote(place, place, send_relay, recv_relay.at[g], (row, across))

    def share(place, kind):
        return remote(place, place, send_share, recv_share.at[kind], (row, sibling))

    def waiter(count, send, recv):
        group = pieces.at[pl.ds(0, count)]
        return remote(group, group, send, recv, (row, sibling))

    def cross(h):
        for level in range(2):
            for g in range(len(groups)):
                for f in range(2):
                    if groups[g][0] == h:
                        far_send(g, level, f).start()

    span = 2 * LANES
    for h in range(HALVES):
        others = pl.ds(0, rows - 1)
        remote(
            packed.at[h, others], arrived.at[h, others], send_one, recv_one.at[h], (row, sibling)
        ).wait_recv()

        def section(t, carry):
            at = pl.multiple_of(t * LANES, LANES)
            x = [arrived[h, r, :, pl.ds(at, LANES)].astype(jnp.float32) for r in range(rows)]
            points = eight_points(x)
            for k in range(POINTS):
                real, imag = points[k]
                if k > 0:
                    cosine = twiddles[0, k : k + 1, pl.ds(at, LANES)]
                    sine = twiddles[1, k : k + 1, pl.ds(at, LANES)]
                    if imag is None:
                        real, imag = real * cosine, -real * sine
                    else:
                        real, imag = real * cosine + imag * sine, imag * cosine - real * sine
                else:
                    imag = jnp.zeros_like(real)
                if h == 1:
                    place = lax.broadcasted_iota(jnp.int32, real.shape, 0) + row * part
                    plain = place == 0
                    real, imag = jnp.where(plain, real, -imag), jnp.where(plain, imag, real)
                stage[k, :, pl.ds(at, LANES)] = real.astype(jnp.bfloat16)
                stage[k, :, pl.ds(pl.multiple_of(block + at, LANES), LANES)] = imag.astype(jnp.bfloat16)
            return carry

        lax.fori_loop(0, block // LANES, section, 0)
        values = stage[...].reshape(POINTS * part, 2 * block)
        def columns(n):
            done = jnp.dot(
                values, table[:, pl.ds(pl.multiple_of(n * span, span), span)], preferred_element_type=jnp.float32
            ).astype(jnp.bfloat16)
            for q in range(2):
                ready[h, 2 * n + q] = done[:, q * LANES : (q + 1) * LANES].reshape(POINTS, part, LANES)

        def nearby():
            for step in range(2):
                columns(mate(2 * step) // 2)
                for d in (2 * step, 2 * step + 1):
                    if d > 0:
                        near_send(h, d).start()
                    direct_send(h, d).start()


        def beyond():
            for level in range(2):
                columns(base_far // 2 + level)
            cross(h)

        for stage_of in (nearby, beyond):
            stage_of()
        gathered[h, col, row] = ready[h, row]

    half_rows = lambda start: pl.ds(start, quarter)

    def relay(g, level):
        for f in range(2):
            far_arrival(g, level, f).wait_recv()
            relay_send(g, level, f).start()

    def share_far(g):
        share(spot(g, col, half_rows(base_far)), HALVES + g).start()

    def pass_on(g):
        place = spot(g, across, half_rows(base_far))
        remote(place, place, send_relay, recv_relay.at[g], (row, across)).wait_recv()
        share(place, HALVES + g).start()

    def share_near(h):
        waiter(quarter - 1, send_near, recv_near.at[h]).wait_recv()
        share(gathered.at[h, col, half_rows(base_near)], h).start()
        waiter(quarter, send_direct, recv_direct.at[h]).wait_recv()
        share(gathered.at[h, across, half_rows(base_near)], h).start()

    depth = cols * quarter * part

    def map_out(h, start, points, fresh):
        weights = folded[h, :, half_rows(start)].reshape(depth, -1)
        for k in points:
            spectrum = gathered[h, :, half_rows(start), k].reshape(depth, LANES)
            piece = lax.dot_general(
                spectrum, weights, (((0,), (0,)), ((), ())), preferred_element_type=jnp.float32
            )
            total[k] = piece if fresh else total[k] + piece

    def map_near(h):
        waiter(rows, send_share, recv_share.at[h]).wait_recv()
        map_out(h, base_near, range(POINTS), h == 0)

    def map_far(g):
        h, first, count = groups[g]
        both = gathered.at[h, pl.ds(0, 2), half_rows(base_far), pl.ds(first, count)]
        remote(both, both, send_share, recv_share.at[HALVES + g], (row, sibling)).wait_recv()
        map_out(h, base_far, range(first, first + count), False)

    inner = 1 - outer
    relay(0, outer)
    relay(0, inner)
    share_far(0)
    share_near(0)
    relay(1, outer)
    relay(1, inner)
    relay(2, outer)
    relay(2, inner)
    for g in range(1, len(groups)):
        share_far(g)
    pass_on(0)
    map_near(0)
    share_near(1)
    map_far(0)
    pass_on(1)
    map_near(1)
    for g in range(2, len(groups)):
        pass_on(g)
    for g in range(1, len(groups)):
        map_far(g)
    out_ref[...] = jnp.swapaxes(total[...], 0, 1).reshape(out_ref.shape).astype(out_ref.dtype)

    others = pl.ds(0, rows - 1)
    remote(packed.at[:, others], arrived.at[:, others], send_one, recv_one.at[0], (row, sibling)).wait_send()
    waiter(HALVES * len(far), send_far, recv_far.at[0, 0]).wait_send()
    waiter(HALVES * (quarter - 1), send_near, recv_near.at[0]).wait_send()
    waiter(HALVES * quarter, send_direct, recv_direct.at[0]).wait_send()
    waiter(HALVES * len(far), send_relay, recv_relay.at[0]).wait_send()
    everything = gathered.at[0]
    remote(everything, everything, send_share, recv_share.at[0], (row, sibling)).wait_send()


def fused(tokens, norm_gain, w_in, w_out):
    rows, cols = lax.axis_size("row"), lax.axis_size("col")
    block, width_in = tokens.shape
    width = w_in.shape[1]
    features = w_out.shape[1]
    part = width // (HALVES * rows)
    marks = (0, 1, 2, 3, 4, 5, 6, 7, 8)
    forward, fold = channel_tables(width, block * rows)
    twiddles, coarse, fine = position_tables(block, block * rows)
    half, short, wide = jnp.bfloat16, pltpu.VMEM, jnp.float32
    operands = [tokens, norm_gain[None, :], w_in, w_out, forward, fold, twiddles, coarse, fine]
    operands = [pltpu.with_memory_space_constraint(jnp.asarray(x), pltpu.HBM) for x in operands]
    dma = pltpu.SemaphoreType.DMA
    groups = ((0, 0, POINTS), (1, 0, POINTS // 2), (1, POINTS // 2, POINTS // 2))
    return pl.pallas_call(
        functools.partial(mixer_kernel, marks, 4, groups),
        out_shape=jax.ShapeDtypeStruct((block, features), half),
        in_specs=[pl.BlockSpec(memory_space=pl.ANY)] * len(operands),
        out_specs=pl.BlockSpec(memory_space=pltpu.VMEM),
        scratch_shapes=[short(x.shape, x.dtype) for x in operands]
        + [
            short((HALVES, rows, part, block), half),
            short((HALVES, rows, part, block), half),
            short((POINTS, part, 2 * block), half),
            short((2 * block, block), half),
            short((HALVES, rows, POINTS, part, LANES), half),
            short((HALVES, cols, rows, POINTS, part, LANES), half),
            short((HALVES, cols, rows, part, features), half),
            short((POINTS, LANES, features), wide),
            short((width_in, LANES), wide),
            dma((len(marks) - 1,)),
            dma((8,)),
            dma(()),
            dma((HALVES,)),
            dma((5,)),
            dma((HALVES,)),
            dma((len(groups), rows // 2)),
            dma((HALVES,)),
            dma((len(groups),)),
            dma((HALVES + len(groups),)),
        ],
        compiler_params=pltpu.CompilerParams(
            collective_id=0, has_side_effects=True, vmem_limit_bytes=32 * 1024 * 1024
        ),
    )(*operands)


def fits(mesh):
    return mesh.shape["row"] == POINTS and mesh.shape["col"] == 4


def choose(mesh, *arrays):
    tokens, _, w_in, _ = arrays
    group_local = w_in.shape[1] == GROUP
    tiles = tokens.shape[0] == POINTS * LANES
    return fused(*arrays) if fits(mesh) and group_local and tiles else local(*arrays)


def solution(mesh):
    placed = (P("row", None), P(), P(None, "col"), P(None, "col"))
    return jax.shard_map(
        functools.partial(choose, mesh), mesh=mesh, in_specs=placed, out_specs=P("row", "col"), check_vma=False
    )
```

```python
import functools
import math

import jax
import jax.numpy as jnp
import numpy as np
from jax import lax
from jax.experimental import pallas as pl
from jax.experimental.pallas import tpu as pltpu
from jax.sharding import PartitionSpec as P

GROUP = 256


NORM_EPS = 1e-06


def as_sent(array):

    def short(part):
        return part.astype(jnp.bfloat16) if part.dtype == jnp.float32 else part

    return jax.tree.map(short, array)


def rotation_table(first_index, second_index, spectral_magnitude, factor):
    phase = (first_index * second_index % spectral_magnitude).astype(jnp.float32) * (
        2.0 * math.pi / spectral_magnitude
    )
    return (jnp.cos(phase) * factor, jnp.sin(phase) * factor)


def twiddle(real_input_values, imag_in, freq_index, pos_index, spectral_magnitude):
    cosine, sine = rotation_table(freq_index, pos_index, spectral_magnitude, 1.0)
    return (
        real_input_values * cosine + imag_in * sine,
        imag_in * cosine - real_input_values * sine,
    )


def second_section(stacked, half):
    length_dev = stacked.shape[1]
    stride = min(length_dev, 512)
    positions = lax.broadcasted_iota(jnp.int32, (length_dev, stride), 0)
    real_blocks = []
    imag_blocks = []
    for offset in range(0, length_dev, stride):
        freqs = lax.broadcasted_iota(jnp.int32, (length_dev, stride), 1) + offset
        cosine, sine = rotation_table(positions, freqs, length_dev, 1.0)
        with_cos = jnp.dot(stacked, cosine, precision=lax.Precision.HIGH)
        with_sin = jnp.dot(stacked, sine, precision=lax.Precision.HIGH)
        real_blocks.append(with_cos[:half] + with_sin[half:])
        imag_blocks.append(with_cos[half:] - with_sin[:half])
    return (jnp.concatenate(real_blocks, 1), jnp.concatenate(imag_blocks, 1))


def reorder_positions(arrived):
    channels, row_count, _, block_len = arrived.shape
    return jnp.swapaxes(arrived.reshape(channels, row_count, block_len), 1, 2).reshape(
        channels, row_count * block_len
    )


def local(tokens, norm_gain, w_in, w_out):
    length_dev = tokens.shape[0]
    row_count = lax.axis_size("row")
    col_count = lax.axis_size("col")
    total_len = length_dev * row_count
    widened = tokens.astype(jnp.float32)
    inverse = lax.rsqrt(jnp.mean(widened * widened, axis=1, keepdims=True) + NORM_EPS)
    normed = (widened * inverse * norm_gain[None, :]).astype(jnp.bfloat16)
    projected = lax.dot_general(
        w_in, normed, (((0,), (1,)), ((), ())), preferred_element_type=jnp.float32
    ).astype(jnp.bfloat16)
    channels = projected.shape[0]
    block_len = length_dev // row_count
    small_cos, small_sin = rotation_table(
        lax.broadcasted_iota(jnp.int32, (row_count, row_count), 0),
        lax.broadcasted_iota(jnp.int32, (row_count, row_count), 1),
        row_count,
        1.0 / math.sqrt(total_len),
    )
    per_row = channels // row_count
    arrived = lax.all_to_all(
        projected.reshape(channels, 1, length_dev), "row", split_axis=0, concat_axis=1, tiled=True
    )
    values = arrived.astype(jnp.float32)
    real_one = jnp.einsum("ka,cab->ckb", small_cos, values, precision=lax.Precision.HIGH)
    imag_one = -jnp.einsum("ka,cab->ckb", small_sin, values, precision=lax.Precision.HIGH)
    freq_index = lax.broadcasted_iota(jnp.int32, (row_count, length_dev), 0)
    pos_index = lax.broadcasted_iota(jnp.int32, (row_count, length_dev), 1)
    real_two, imag_two = twiddle(real_one, imag_one, freq_index, pos_index, total_len)
    stacked = jnp.concatenate(
        [
            real_two.reshape(per_row * row_count, length_dev),
            imag_two.reshape(per_row * row_count, length_dev),
        ],
        0,
    )
    real_three, imag_three = second_section(stacked, per_row * row_count)
    shaped = (per_row, row_count, row_count, block_len)
    back_real, back_imag = (
        lax.all_to_all(
            real_three.reshape(shaped).astype(jnp.bfloat16),
            "row",
            split_axis=2,
            concat_axis=0,
            tiled=True,
        ).astype(jnp.float32),
        lax.all_to_all(
            imag_three.reshape(shaped).astype(jnp.bfloat16),
            "row",
            split_axis=2,
            concat_axis=0,
            tiled=True,
        ).astype(jnp.float32),
    )
    spec_real = reorder_positions(back_real)
    spec_imag = reorder_positions(back_imag)
    quarter = length_dev // col_count
    group_cosine_table, group_sine_table = rotation_table(
        lax.broadcasted_iota(jnp.int32, (GROUP, GROUP), 0),
        lax.broadcasted_iota(jnp.int32, (GROUP, GROUP), 1),
        GROUP,
        1.0 / math.sqrt(GROUP),
    )
    real_input_values = lax.all_to_all(
        as_sent(spec_real.reshape(channels, col_count, quarter)),
        "col",
        split_axis=1,
        concat_axis=0,
        tiled=True,
    )
    imag_in = lax.all_to_all(
        as_sent(spec_imag.reshape(channels, col_count, quarter)),
        "col",
        split_axis=1,
        concat_axis=0,
        tiled=True,
    )
    width_all = real_input_values.shape[0]
    item_count = real_input_values.shape[2]
    groups = width_all // GROUP
    real_by_group = real_input_values.reshape(groups, GROUP, item_count)
    imaginary_by_group = imag_in.reshape(groups, GROUP, item_count)
    merged_spectrum = jnp.einsum(
        "hz,azo->aho", group_cosine_table, real_by_group, precision=lax.Precision.HIGH
    )
    merged_spectrum = merged_spectrum + jnp.einsum(
        "hz,azo->aho", group_sine_table, imaginary_by_group, precision=lax.Precision.HIGH
    )
    result = merged_spectrum.reshape(width_all, 1, item_count).astype(jnp.bfloat16)
    spectral = lax.all_to_all(result, "col", split_axis=0, concat_axis=1, tiled=True)
    output = lax.dot_general(
        lax.all_gather(spectral.reshape(channels, length_dev), "col", axis=0, tiled=True),
        w_out,
        (((0,), (0,)), ((), ())),
        preferred_element_type=jnp.float32,
    )
    return output.astype(jnp.bfloat16)


HALVES = 2
POINTS = 8
LANES = 128
MESH = pl.DeviceIdType.MESH


def channel_tables(group, total_len):
    half = group // 2
    index = np.arange(group)
    angle = 2.0 * np.pi * (index[:, None] * index[None, :] % group) / group
    transform = np.concatenate([np.cos(angle[: half + 1]), np.sin(angle[1:half])], 0)
    fold = np.zeros((group, group))
    for k in range(half + 1):
        fold[k, k] = 1.0
        fold[k, -k % group] = 1.0
    for k in range(1, half):
        fold[half + k, group - k] = 1.0
        fold[half + k, k] = -1.0
    return (transform / math.sqrt(group)).astype(jnp.bfloat16), fold.astype(jnp.bfloat16)


def position_tables(block, total_len):
    j = np.arange(block)
    angle = 2.0 * np.pi * (np.arange(POINTS)[:, None] * j[None, :]) / total_len
    twiddles = np.stack([np.cos(angle), np.sin(angle)]).astype(np.float32)
    root = 32
    coarse = 2.0 * np.pi * (np.arange(block // root)[:, None] * root * j[None, :] % block) / block
    fine = 2.0 * np.pi * (np.arange(root)[:, None] * j[None, :] % block) / block
    scale = 1.0 / math.sqrt(total_len)
    coarse = np.stack([np.cos(coarse), np.sin(coarse)]).astype(np.float32)
    fine = np.stack([np.cos(fine) * scale, np.sin(fine) * scale]).astype(np.float32)
    return twiddles, coarse, fine


def eight_points(x):
    a = [x[i] + x[i + 4] for i in range(4)]
    b = [x[i] - x[i + 4] for i in range(4)]
    even, odd = a[0] + a[2], a[1] + a[3]
    root = math.sqrt(0.5)
    minus, plus = root * (b[1] - b[3]), root * (b[1] + b[3])
    one = (b[0] + minus, -b[2] - plus)
    two = (a[0] - a[2], a[3] - a[1])
    three = (b[0] - minus, b[2] - plus)
    return [
        (even + odd, None),
        one,
        two,
        three,
        (even - odd, None),
        (three[0], -three[1]),
        (two[0], -two[1]),
        (one[0], -one[1]),
    ]


def mixer_kernel(
    marks, ahead, groups,
    tokens_hbm, gain_hbm, w_in_hbm, w_out_hbm, forward_hbm, fold_hbm, twiddle_hbm, coarse_hbm, fine_hbm,
    out_ref,
    tokens, gain, w_in, w_out, forward, fold, twiddles, coarse, fine,
    packed, arrived, stage, table, ready, gathered, folded, total, spread,
    token_sem, load_sem, send_one, recv_one, send_two, recv_near, recv_far, recv_direct, recv_relay, recv_share,
):
    row, col = lax.axis_index("row"), lax.axis_index("col")
    rows = packed.shape[1]
    block, width = packed.shape[3], w_in.shape[1]
    edges = [block // LANES * LANES * i // 8 for i in marks]
    chunks = [pl.ds(a, b - a) for a, b in zip(edges, edges[1:])]
    steps = len(chunks)
    part = packed.shape[2]
    flip = lambda index, bit: index + bit - 2 * bit * (index // bit % 2)
    sibling, across = flip(col, 1), flip(col, 2)
    quarter = rows // 2
    near, far = list(range(quarter)), list(range(quarter, rows))

    def mate(d):
        index = row
        for bit in (1, 2, 4):
            if d & bit:
                index = flip(index, bit)
        return index

    loads = [
        pltpu.make_async_copy(src, dst, load_sem.at[i])
        for i, (src, dst) in enumerate([
            (w_in_hbm, w_in), (gain_hbm, gain), (forward_hbm, forward), (coarse_hbm, coarse), (fine_hbm, fine),
            (twiddle_hbm, twiddles), (fold_hbm, fold), (w_out_hbm, w_out),
        ])
    ]
    token_loads = [
        pltpu.make_async_copy(tokens_hbm.at[where], tokens.at[where], token_sem.at[p])
        for p, where in enumerate(chunks)
    ]
    for load in [loads[1], loads[0], token_loads[0], loads[2]] + token_loads[1:ahead]:
        load.start()

    barrier = pltpu.get_barrier_semaphore()
    peers = [(mate(d), col) for d in range(1, rows)] + [(row, sibling)]
    peers += [(mate(d), across) for d in near]
    for peer in peers:
        pl.semaphore_signal(barrier, inc=1, device_id=peer, device_id_type=MESH)

    def remote(src, dst, send, recv, device):
        return pltpu.make_async_remote_copy(
            src_ref=src, dst_ref=dst, send_sem=send, recv_sem=recv, device_id=device, device_id_type=MESH
        )

    def first_send(h, d, where):
        peer = mate(d)
        return remote(
            packed.at[h, peer, :, where], arrived.at[h, row, :, where], send_one, recv_one.at[h], (peer, col)
        )

    order = far + [2, 3, 1]
    edge = row // 2 % 3 == 0
    loads[1].wait()
    across_lanes = [
        jnp.transpose(jnp.broadcast_to(gain[:, i : i + LANES], (LANES, LANES)))
        for i in range(0, gain.shape[1], LANES)
    ]
    for i, scale in enumerate(across_lanes):
        spread[i * LANES : (i + 1) * LANES, :] = scale
    loads[0].wait()
    for i in range(0, width, LANES):
        lanes = slice(i, i + LANES)
        w_in[:, lanes] = (w_in[:, lanes].astype(jnp.float32) * spread[...]).astype(jnp.bfloat16)
    loads[2].wait()
    for p, where in enumerate(chunks):
        token_loads[p].wait()
        if p + ahead < steps:
            token_loads[p + ahead].start()
        elif p + ahead == steps:
            for load in loads[3:]:
                load.start()
        piece = tokens[where, :]
        wide = piece.astype(jnp.float32)
        inverse = lax.rsqrt(jnp.mean(wide * wide, axis=1, keepdims=True) + NORM_EPS)
        projected = jnp.dot(piece, w_in[...], preferred_element_type=jnp.float32)
        projected = (projected * inverse).astype(jnp.bfloat16)
        kept = lax.dot_general(
            forward[...], projected, (((1,), (1,)), ((), ())), preferred_element_type=jnp.float32
        )
        packed[:, :, :, where] = kept.astype(jnp.bfloat16).reshape(HALVES, rows, part, where.size)
        if p == 0:
            pl.semaphore_wait(barrier, len(peers))
        for d in order:
            first_send(0, d, where).start()
    def second_half():
        for d in order:
            first_send(1, d, pl.ds(0, block)).start()

    second_half()
    for h in range(HALVES):
        arrived[h, row] = packed[h, row]
    for load in loads[3:]:
        load.wait()

    root = fine.shape[1]

    def table_rows(a, carry):
        cos_a, sin_a = coarse[0, pl.ds(a, 1), :], coarse[1, pl.ds(a, 1), :]
        at = pl.multiple_of(a * root, root)
        table[pl.ds(at, root), :] = (cos_a * fine[0] - sin_a * fine[1]).astype(jnp.bfloat16)
        table[pl.ds(block + at, root), :] = (sin_a * fine[0] + cos_a * fine[1]).astype(jnp.bfloat16)
        return carry

    lax.fori_loop(0, block // root, table_rows, 0)
    cols = w_out.shape[0] // width
    half = width // HALVES
    for c in range(cols):
        rows_out = jnp.dot(
            fold[...], w_out[c * width : (c + 1) * width, :], preferred_element_type=jnp.float32
        ).astype(jnp.bfloat16)
        for h in range(HALVES):
            folded[h, c] = rows_out[h * half : (h + 1) * half].reshape(rows, part, -1)

    base_near = row // quarter * quarter
    base_far = quarter - base_near
    outer = base_far // quarter
    pieces = gathered.at[0, 0]
    send_far, send_near, send_direct, send_relay, send_share = (send_two.at[i] for i in range(5))

    def near_send(h, d):
        return remote(ready.at[h, mate(d)], gathered.at[h, col, row], send_near, recv_near.at[h], (mate(d), col))

    def direct_send(h, d):
        return remote(
            ready.at[h, mate(d)], gathered.at[h, col, row], send_direct, recv_direct.at[h], (mate(d), across)
        )

    def spot(g, owner, place):
        h, first, count = groups[g]
        return gathered.at[h, owner, place, pl.ds(first, count)]

    def crossing(level, f):
        return base_far + 2 * level + flip(row % 2, f)

    def far_send(g, level, f):
        h, first, count = groups[g]
        peer = crossing(level, f)
        return remote(
            ready.at[h, peer, pl.ds(first, count)], spot(g, col, row),
            send_far, recv_far.at[g, row % quarter], (peer, col),
        )

    def far_arrival(g, level, f):
        source = crossing(level, f)
        place = spot(g, col, source)
        return remote(place, place, send_far, recv_far.at[g, source % quarter], (source, col))

    def relay_send(g, level, f):
        place = spot(g, col, crossing(level, f))
        return remote(place, place, send_relay, recv_relay.at[g], (row, across))

    def share(place, kind):
        return remote(place, place, send_share, recv_share.at[kind], (row, sibling))

    def waiter(count, send, recv):
        group = pieces.at[pl.ds(0, count)]
        return remote(group, group, send, recv, (row, sibling))

    def cross(h):
        for level in range(2):
            for g in range(len(groups)):
                for f in range(2):
                    if groups[g][0] == h:
                        far_send(g, level, f).start()

    span = 2 * LANES
    for h in range(HALVES):
        others = pl.ds(0, rows - 1)
        remote(
            packed.at[h, others], arrived.at[h, others], send_one, recv_one.at[h], (row, sibling)
        ).wait_recv()

        def section(t, carry):
            at = pl.multiple_of(t * LANES, LANES)
            x = [arrived[h, r, :, pl.ds(at, LANES)].astype(jnp.float32) for r in range(rows)]
            points = eight_points(x)
            for k in range(POINTS):
                real, imag = points[k]
                if k > 0:
                    cosine = twiddles[0, k : k + 1, pl.ds(at, LANES)]
                    sine = twiddles[1, k : k + 1, pl.ds(at, LANES)]
                    if imag is None:
                        real, imag = real * cosine, -real * sine
                    else:
                        real, imag = real * cosine + imag * sine, imag * cosine - real * sine
                else:
                    imag = jnp.zeros_like(real)
                if h == 1:
                    place = lax.broadcasted_iota(jnp.int32, real.shape, 0) + row * part
                    plain = place == 0
                    real, imag = jnp.where(plain, real, -imag), jnp.where(plain, imag, real)
                stage[k, :, pl.ds(at, LANES)] = real.astype(jnp.bfloat16)
                stage[k, :, pl.ds(pl.multiple_of(block + at, LANES), LANES)] = imag.astype(jnp.bfloat16)
            return carry

        lax.fori_loop(0, block // LANES, section, 0)
        values = stage[...].reshape(POINTS * part, 2 * block)
        def columns(n):
            done = jnp.dot(
                values, table[:, pl.ds(pl.multiple_of(n * span, span), span)], preferred_element_type=jnp.float32
            ).astype(jnp.bfloat16)
            for q in range(2):
                ready[h, 2 * n + q] = done[:, q * LANES : (q + 1) * LANES].reshape(POINTS, part, LANES)

        def nearby():
            for step in range(2):
                columns(mate(2 * step) // 2)
                for d in (2 * step, 2 * step + 1):
                    if d > 0:
                        near_send(h, d).start()
                    direct_send(h, d).start()


        def beyond():
            for level in range(2):
                columns(base_far // 2 + level)
            cross(h)

        for stage_of in (nearby, beyond):
            stage_of()
        gathered[h, col, row] = ready[h, row]

    half_rows = lambda start: pl.ds(start, quarter)

    def relay(g, level):
        for f in range(2):
            far_arrival(g, level, f).wait_recv()
            relay_send(g, level, f).start()

    def share_far(g):
        share(spot(g, col, half_rows(base_far)), HALVES + g).start()

    def pass_on(g):
        place = spot(g, across, half_rows(base_far))
        remote(place, place, send_relay, recv_relay.at[g], (row, across)).wait_recv()
        share(place, HALVES + g).start()

    def share_near(h):
        waiter(quarter - 1, send_near, recv_near.at[h]).wait_recv()
        share(gathered.at[h, col, half_rows(base_near)], h).start()
        waiter(quarter, send_direct, recv_direct.at[h]).wait_recv()
        share(gathered.at[h, across, half_rows(base_near)], h).start()

    depth = cols * quarter * part

    def map_out(h, start, points, fresh):
        weights = folded[h, :, half_rows(start)].reshape(depth, -1)
        for k in points:
            spectrum = gathered[h, :, half_rows(start), k].reshape(depth, LANES)
            piece = lax.dot_general(
                spectrum, weights, (((0,), (0,)), ((), ())), preferred_element_type=jnp.float32
            )
            total[k] = piece if fresh else total[k] + piece

    def map_near(h):
        waiter(rows, send_share, recv_share.at[h]).wait_recv()
        map_out(h, base_near, range(POINTS), h == 0)

    def map_far(g):
        h, first, count = groups[g]
        both = gathered.at[h, pl.ds(0, 2), half_rows(base_far), pl.ds(first, count)]
        remote(both, both, send_share, recv_share.at[HALVES + g], (row, sibling)).wait_recv()
        map_out(h, base_far, range(first, first + count), False)

    inner = 1 - outer
    relay(0, outer)
    relay(0, inner)
    share_far(0)
    share_near(0)
    relay(1, outer)
    relay(1, inner)
    relay(2, outer)
    relay(2, inner)
    relay(3, outer)
    relay(3, inner)
    for g in range(1, len(groups)):
        share_far(g)
    pass_on(0)
    map_near(0)
    share_near(1)
    map_far(0)
    pass_on(1)
    map_near(1)
    for g in range(2, len(groups)):
        pass_on(g)
    for g in range(1, len(groups)):
        map_far(g)
    out_ref[...] = jnp.swapaxes(total[...], 0, 1).reshape(out_ref.shape).astype(out_ref.dtype)

    others = pl.ds(0, rows - 1)
    remote(packed.at[:, others], arrived.at[:, others], send_one, recv_one.at[0], (row, sibling)).wait_send()
    waiter(HALVES * len(far), send_far, recv_far.at[0, 0]).wait_send()
    waiter(HALVES * (quarter - 1), send_near, recv_near.at[0]).wait_send()
    waiter(HALVES * quarter, send_direct, recv_direct.at[0]).wait_send()
    waiter(HALVES * len(far), send_relay, recv_relay.at[0]).wait_send()
    everything = gathered.at[0]
    remote(everything, everything, send_share, recv_share.at[0], (row, sibling)).wait_send()


def fused(tokens, norm_gain, w_in, w_out):
    rows, cols = lax.axis_size("row"), lax.axis_size("col")
    block, width_in = tokens.shape
    width = w_in.shape[1]
    features = w_out.shape[1]
    part = width // (HALVES * rows)
    marks = (0, 1, 2, 3, 4, 5, 6, 7, 8)
    forward, fold = channel_tables(width, block * rows)
    twiddles, coarse, fine = position_tables(block, block * rows)
    half, short, wide = jnp.bfloat16, pltpu.VMEM, jnp.float32
    operands = [tokens, norm_gain[None, :], w_in, w_out, forward, fold, twiddles, coarse, fine]
    operands = [pltpu.with_memory_space_constraint(jnp.asarray(x), pltpu.HBM) for x in operands]
    dma = pltpu.SemaphoreType.DMA
    quad = POINTS // 4
    groups = ((0, 0, POINTS), (1, 0, 2 * quad), (1, 2 * quad, quad), (1, 3 * quad, quad))
    return pl.pallas_call(
        functools.partial(mixer_kernel, marks, 4, groups),
        out_shape=jax.ShapeDtypeStruct((block, features), half),
        in_specs=[pl.BlockSpec(memory_space=pl.ANY)] * len(operands),
        out_specs=pl.BlockSpec(memory_space=pltpu.VMEM),
        scratch_shapes=[short(x.shape, x.dtype) for x in operands]
        + [
            short((HALVES, rows, part, block), half),
            short((HALVES, rows, part, block), half),
            short((POINTS, part, 2 * block), half),
            short((2 * block, block), half),
            short((HALVES, rows, POINTS, part, LANES), half),
            short((HALVES, cols, rows, POINTS, part, LANES), half),
            short((HALVES, cols, rows, part, features), half),
            short((POINTS, LANES, features), wide),
            short((width_in, LANES), wide),
            dma((len(marks) - 1,)),
            dma((8,)),
            dma(()),
            dma((HALVES,)),
            dma((5,)),
            dma((HALVES,)),
            dma((len(groups), rows // 2)),
            dma((HALVES,)),
            dma((len(groups),)),
            dma((HALVES + len(groups),)),
        ],
        compiler_params=pltpu.CompilerParams(
            collective_id=0, has_side_effects=True, vmem_limit_bytes=32 * 1024 * 1024
        ),
    )(*operands)


def fits(mesh):
    return mesh.shape["row"] == POINTS and mesh.shape["col"] == 4


def choose(mesh, *arrays):
    tokens, _, w_in, _ = arrays
    group_local = w_in.shape[1] == GROUP
    tiles = tokens.shape[0] == POINTS * LANES
    return fused(*arrays) if fits(mesh) and group_local and tiles else local(*arrays)


def solution(mesh):
    placed = (P("row", None), P(), P(None, "col"), P(None, "col"))
    return jax.shard_map(
        functools.partial(choose, mesh), mesh=mesh, in_specs=placed, out_specs=P("row", "col"), check_vma=False
    )
```

```python
import functools
import math

import jax
import jax.numpy as jnp
import numpy as np
from jax import lax
from jax.experimental import pallas as pl
from jax.experimental.pallas import tpu as pltpu
from jax.sharding import PartitionSpec as P

GROUP = 256


NORM_EPS = 1e-06


def as_sent(array):

    def short(part):
        return part.astype(jnp.bfloat16) if part.dtype == jnp.float32 else part

    return jax.tree.map(short, array)


def rotation_table(first_index, second_index, spectral_magnitude, factor):
    phase = (first_index * second_index % spectral_magnitude).astype(jnp.float32) * (
        2.0 * math.pi / spectral_magnitude
    )
    return (jnp.cos(phase) * factor, jnp.sin(phase) * factor)


def twiddle(real_input_values, imag_in, freq_index, pos_index, spectral_magnitude):
    cosine, sine = rotation_table(freq_index, pos_index, spectral_magnitude, 1.0)
    return (
        real_input_values * cosine + imag_in * sine,
        imag_in * cosine - real_input_values * sine,
    )


def second_section(stacked, half):
    length_dev = stacked.shape[1]
    stride = min(length_dev, 512)
    positions = lax.broadcasted_iota(jnp.int32, (length_dev, stride), 0)
    real_blocks = []
    imag_blocks = []
    for offset in range(0, length_dev, stride):
        freqs = lax.broadcasted_iota(jnp.int32, (length_dev, stride), 1) + offset
        cosine, sine = rotation_table(positions, freqs, length_dev, 1.0)
        with_cos = jnp.dot(stacked, cosine, precision=lax.Precision.HIGH)
        with_sin = jnp.dot(stacked, sine, precision=lax.Precision.HIGH)
        real_blocks.append(with_cos[:half] + with_sin[half:])
        imag_blocks.append(with_cos[half:] - with_sin[:half])
    return (jnp.concatenate(real_blocks, 1), jnp.concatenate(imag_blocks, 1))


def reorder_positions(arrived):
    channels, row_count, _, block_len = arrived.shape
    return jnp.swapaxes(arrived.reshape(channels, row_count, block_len), 1, 2).reshape(
        channels, row_count * block_len
    )


def local(tokens, norm_gain, w_in, w_out):
    length_dev = tokens.shape[0]
    row_count = lax.axis_size("row")
    col_count = lax.axis_size("col")
    total_len = length_dev * row_count
    widened = tokens.astype(jnp.float32)
    inverse = lax.rsqrt(jnp.mean(widened * widened, axis=1, keepdims=True) + NORM_EPS)
    normed = (widened * inverse * norm_gain[None, :]).astype(jnp.bfloat16)
    projected = lax.dot_general(
        w_in, normed, (((0,), (1,)), ((), ())), preferred_element_type=jnp.float32
    ).astype(jnp.bfloat16)
    channels = projected.shape[0]
    block_len = length_dev // row_count
    small_cos, small_sin = rotation_table(
        lax.broadcasted_iota(jnp.int32, (row_count, row_count), 0),
        lax.broadcasted_iota(jnp.int32, (row_count, row_count), 1),
        row_count,
        1.0 / math.sqrt(total_len),
    )
    per_row = channels // row_count
    arrived = lax.all_to_all(
        projected.reshape(channels, 1, length_dev), "row", split_axis=0, concat_axis=1, tiled=True
    )
    values = arrived.astype(jnp.float32)
    real_one = jnp.einsum("ka,cab->ckb", small_cos, values, precision=lax.Precision.HIGH)
    imag_one = -jnp.einsum("ka,cab->ckb", small_sin, values, precision=lax.Precision.HIGH)
    freq_index = lax.broadcasted_iota(jnp.int32, (row_count, length_dev), 0)
    pos_index = lax.broadcasted_iota(jnp.int32, (row_count, length_dev), 1)
    real_two, imag_two = twiddle(real_one, imag_one, freq_index, pos_index, total_len)
    stacked = jnp.concatenate(
        [
            real_two.reshape(per_row * row_count, length_dev),
            imag_two.reshape(per_row * row_count, length_dev),
        ],
        0,
    )
    real_three, imag_three = second_section(stacked, per_row * row_count)
    shaped = (per_row, row_count, row_count, block_len)
    back_real, back_imag = (
        lax.all_to_all(
            real_three.reshape(shaped).astype(jnp.bfloat16),
            "row",
            split_axis=2,
            concat_axis=0,
            tiled=True,
        ).astype(jnp.float32),
        lax.all_to_all(
            imag_three.reshape(shaped).astype(jnp.bfloat16),
            "row",
            split_axis=2,
            concat_axis=0,
            tiled=True,
        ).astype(jnp.float32),
    )
    spec_real = reorder_positions(back_real)
    spec_imag = reorder_positions(back_imag)
    quarter = length_dev // col_count
    group_cosine_table, group_sine_table = rotation_table(
        lax.broadcasted_iota(jnp.int32, (GROUP, GROUP), 0),
        lax.broadcasted_iota(jnp.int32, (GROUP, GROUP), 1),
        GROUP,
        1.0 / math.sqrt(GROUP),
    )
    real_input_values = lax.all_to_all(
        as_sent(spec_real.reshape(channels, col_count, quarter)),
        "col",
        split_axis=1,
        concat_axis=0,
        tiled=True,
    )
    imag_in = lax.all_to_all(
        as_sent(spec_imag.reshape(channels, col_count, quarter)),
        "col",
        split_axis=1,
        concat_axis=0,
        tiled=True,
    )
    width_all = real_input_values.shape[0]
    item_count = real_input_values.shape[2]
    groups = width_all // GROUP
    real_by_group = real_input_values.reshape(groups, GROUP, item_count)
    imaginary_by_group = imag_in.reshape(groups, GROUP, item_count)
    merged_spectrum = jnp.einsum(
        "hz,azo->aho", group_cosine_table, real_by_group, precision=lax.Precision.HIGH
    )
    merged_spectrum = merged_spectrum + jnp.einsum(
        "hz,azo->aho", group_sine_table, imaginary_by_group, precision=lax.Precision.HIGH
    )
    result = merged_spectrum.reshape(width_all, 1, item_count).astype(jnp.bfloat16)
    spectral = lax.all_to_all(result, "col", split_axis=0, concat_axis=1, tiled=True)
    output = lax.dot_general(
        lax.all_gather(spectral.reshape(channels, length_dev), "col", axis=0, tiled=True),
        w_out,
        (((0,), (0,)), ((), ())),
        preferred_element_type=jnp.float32,
    )
    return output.astype(jnp.bfloat16)


HALVES = 2
POINTS = 8
LANES = 128
MESH = pl.DeviceIdType.MESH


def channel_tables(group, total_len):
    half = group // 2
    index = np.arange(group)
    angle = 2.0 * np.pi * (index[:, None] * index[None, :] % group) / group
    transform = np.concatenate([np.cos(angle[: half + 1]), np.sin(angle[1:half])], 0)
    fold = np.zeros((group, group))
    for k in range(half + 1):
        fold[k, k] = 1.0
        fold[k, -k % group] = 1.0
    for k in range(1, half):
        fold[half + k, group - k] = 1.0
        fold[half + k, k] = -1.0
    return (transform / math.sqrt(group)).astype(jnp.bfloat16), fold.astype(jnp.bfloat16)


def position_tables(block, total_len):
    j = np.arange(block)
    angle = 2.0 * np.pi * (np.arange(POINTS)[:, None] * j[None, :]) / total_len
    twiddles = np.stack([np.cos(angle), np.sin(angle)]).astype(np.float32)
    root = 32
    coarse = 2.0 * np.pi * (np.arange(block // root)[:, None] * root * j[None, :] % block) / block
    fine = 2.0 * np.pi * (np.arange(root)[:, None] * j[None, :] % block) / block
    scale = 1.0 / math.sqrt(total_len)
    coarse = np.stack([np.cos(coarse), np.sin(coarse)]).astype(np.float32)
    fine = np.stack([np.cos(fine) * scale, np.sin(fine) * scale]).astype(np.float32)
    return twiddles, coarse, fine


def eight_points(x):
    a = [x[i] + x[i + 4] for i in range(4)]
    b = [x[i] - x[i + 4] for i in range(4)]
    even, odd = a[0] + a[2], a[1] + a[3]
    root = math.sqrt(0.5)
    minus, plus = root * (b[1] - b[3]), root * (b[1] + b[3])
    one = (b[0] + minus, -b[2] - plus)
    two = (a[0] - a[2], a[3] - a[1])
    three = (b[0] - minus, b[2] - plus)
    return [
        (even + odd, None),
        one,
        two,
        three,
        (even - odd, None),
        (three[0], -three[1]),
        (two[0], -two[1]),
        (one[0], -one[1]),
    ]


def mixer_kernel(
    marks, ahead, groups,
    tokens_hbm, gain_hbm, w_in_hbm, w_out_hbm, forward_hbm, fold_hbm, twiddle_hbm, coarse_hbm, fine_hbm,
    out_ref,
    tokens, gain, w_in, w_out, forward, fold, twiddles, coarse, fine,
    packed, arrived, stage, table, ready, gathered, folded, total, spread,
    token_sem, load_sem, send_one, recv_one, send_two, recv_near, recv_far, recv_direct, recv_relay, recv_share,
):
    row, col = lax.axis_index("row"), lax.axis_index("col")
    rows = packed.shape[1]
    block, width = packed.shape[3], w_in.shape[1]
    edges = [block // LANES * LANES * i // 8 for i in marks]
    chunks = [pl.ds(a, b - a) for a, b in zip(edges, edges[1:])]
    steps = len(chunks)
    part = packed.shape[2]
    flip = lambda index, bit: index + bit - 2 * bit * (index // bit % 2)
    sibling, across = flip(col, 1), flip(col, 2)
    quarter = rows // 2
    near, far = list(range(quarter)), list(range(quarter, rows))

    def mate(d):
        index = row
        for bit in (1, 2, 4):
            if d & bit:
                index = flip(index, bit)
        return index

    loads = [
        pltpu.make_async_copy(src, dst, load_sem.at[i])
        for i, (src, dst) in enumerate([
            (w_in_hbm, w_in), (gain_hbm, gain), (forward_hbm, forward), (coarse_hbm, coarse), (fine_hbm, fine),
            (twiddle_hbm, twiddles), (fold_hbm, fold), (w_out_hbm, w_out),
        ])
    ]
    token_loads = [
        pltpu.make_async_copy(tokens_hbm.at[where], tokens.at[where], token_sem.at[p])
        for p, where in enumerate(chunks)
    ]
    for load in [loads[1], loads[0], token_loads[0], loads[2]] + token_loads[1:ahead]:
        load.start()

    barrier = pltpu.get_barrier_semaphore()
    peers = [(mate(d), col) for d in range(1, rows)] + [(row, sibling)]
    peers += [(mate(d), across) for d in near]
    for peer in peers:
        pl.semaphore_signal(barrier, inc=1, device_id=peer, device_id_type=MESH)

    def remote(src, dst, send, recv, device):
        return pltpu.make_async_remote_copy(
            src_ref=src, dst_ref=dst, send_sem=send, recv_sem=recv, device_id=device, device_id_type=MESH
        )

    def first_send(h, d, where):
        peer = mate(d)
        return remote(
            packed.at[h, peer, :, where], arrived.at[h, row, :, where], send_one, recv_one.at[h], (peer, col)
        )

    order = far + [2, 3, 1]
    edge = row // 2 % 3 == 0
    loads[1].wait()
    across_lanes = [
        jnp.transpose(jnp.broadcast_to(gain[:, i : i + LANES], (LANES, LANES)))
        for i in range(0, gain.shape[1], LANES)
    ]
    for i, scale in enumerate(across_lanes):
        spread[i * LANES : (i + 1) * LANES, :] = scale
    loads[0].wait()
    for i in range(0, width, LANES):
        lanes = slice(i, i + LANES)
        w_in[:, lanes] = (w_in[:, lanes].astype(jnp.float32) * spread[...]).astype(jnp.bfloat16)
    loads[2].wait()
    for p, where in enumerate(chunks):
        token_loads[p].wait()
        if p + ahead < steps:
            token_loads[p + ahead].start()
        elif p + ahead == steps:
            for load in loads[3:]:
                load.start()
        piece = tokens[where, :]
        wide = piece.astype(jnp.float32)
        inverse = lax.rsqrt(jnp.mean(wide * wide, axis=1, keepdims=True) + NORM_EPS)
        projected = jnp.dot(piece, w_in[...], preferred_element_type=jnp.float32)
        projected = (projected * inverse).astype(jnp.bfloat16)
        kept = lax.dot_general(
            forward[...], projected, (((1,), (1,)), ((), ())), preferred_element_type=jnp.float32
        )
        packed[:, :, :, where] = kept.astype(jnp.bfloat16).reshape(HALVES, rows, part, where.size)
        if p == 0:
            pl.semaphore_wait(barrier, len(peers))
        for d in order:
            first_send(0, d, where).start()
    def second_half():
        for d in [2, 3, 1] + far:
            first_send(1, d, pl.ds(0, block)).start()

    second_half()
    for h in range(HALVES):
        arrived[h, row] = packed[h, row]
    for load in loads[3:]:
        load.wait()

    root = fine.shape[1]

    def table_rows(a, carry):
        cos_a, sin_a = coarse[0, pl.ds(a, 1), :], coarse[1, pl.ds(a, 1), :]
        at = pl.multiple_of(a * root, root)
        table[pl.ds(at, root), :] = (cos_a * fine[0] - sin_a * fine[1]).astype(jnp.bfloat16)
        table[pl.ds(block + at, root), :] = (sin_a * fine[0] + cos_a * fine[1]).astype(jnp.bfloat16)
        return carry

    lax.fori_loop(0, block // root, table_rows, 0)
    cols = w_out.shape[0] // width
    half = width // HALVES
    for c in range(cols):
        rows_out = jnp.dot(
            fold[...], w_out[c * width : (c + 1) * width, :], preferred_element_type=jnp.float32
        ).astype(jnp.bfloat16)
        for h in range(HALVES):
            folded[h, c] = rows_out[h * half : (h + 1) * half].reshape(rows, part, -1)

    base_near = row // quarter * quarter
    base_far = quarter - base_near
    outer = base_far // quarter
    pieces = gathered.at[0, 0]
    send_far, send_near, send_direct, send_relay, send_share = (send_two.at[i] for i in range(5))

    def near_send(h, d):
        return remote(ready.at[h, mate(d)], gathered.at[h, col, row], send_near, recv_near.at[h], (mate(d), col))

    def direct_send(h, d):
        return remote(
            ready.at[h, mate(d)], gathered.at[h, col, row], send_direct, recv_direct.at[h], (mate(d), across)
        )

    def spot(g, owner, place):
        h, first, count = groups[g]
        return gathered.at[h, owner, place, pl.ds(first, count)]

    def crossing(level, f):
        return base_far + 2 * level + flip(row % 2, f)

    def far_send(g, level, f):
        h, first, count = groups[g]
        peer = crossing(level, f)
        return remote(
            ready.at[h, peer, pl.ds(first, count)], spot(g, col, row),
            send_far, recv_far.at[g, row % quarter], (peer, col),
        )

    def far_arrival(g, level, f):
        source = crossing(level, f)
        place = spot(g, col, source)
        return remote(place, place, send_far, recv_far.at[g, source % quarter], (source, col))

    def relay_send(g, level, f):
        place = spot(g, col, crossing(level, f))
        return remote(place, place, send_relay, recv_relay.at[g], (row, across))

    def share(place, kind):
        return remote(place, place, send_share, recv_share.at[kind], (row, sibling))

    def waiter(count, send, recv):
        group = pieces.at[pl.ds(0, count)]
        return remote(group, group, send, recv, (row, sibling))

    def cross(h):
        for level in range(2):
            for g in range(len(groups)):
                for f in range(2):
                    if groups[g][0] == h:
                        far_send(g, level, f).start()

    span = 2 * LANES
    for h in range(HALVES):
        others = pl.ds(0, rows - 1)
        remote(
            packed.at[h, others], arrived.at[h, others], send_one, recv_one.at[h], (row, sibling)
        ).wait_recv()

        def section(t, carry):
            at = pl.multiple_of(t * LANES, LANES)
            x = [arrived[h, r, :, pl.ds(at, LANES)].astype(jnp.float32) for r in range(rows)]
            points = eight_points(x)
            for k in range(POINTS):
                real, imag = points[k]
                if k > 0:
                    cosine = twiddles[0, k : k + 1, pl.ds(at, LANES)]
                    sine = twiddles[1, k : k + 1, pl.ds(at, LANES)]
                    if imag is None:
                        real, imag = real * cosine, -real * sine
                    else:
                        real, imag = real * cosine + imag * sine, imag * cosine - real * sine
                else:
                    imag = jnp.zeros_like(real)
                if h == 1:
                    place = lax.broadcasted_iota(jnp.int32, real.shape, 0) + row * part
                    plain = place == 0
                    real, imag = jnp.where(plain, real, -imag), jnp.where(plain, imag, real)
                stage[k, :, pl.ds(at, LANES)] = real.astype(jnp.bfloat16)
                stage[k, :, pl.ds(pl.multiple_of(block + at, LANES), LANES)] = imag.astype(jnp.bfloat16)
            return carry

        lax.fori_loop(0, block // LANES, section, 0)
        values = stage[...].reshape(POINTS * part, 2 * block)
        def columns(n):
            done = jnp.dot(
                values, table[:, pl.ds(pl.multiple_of(n * span, span), span)], preferred_element_type=jnp.float32
            ).astype(jnp.bfloat16)
            for q in range(2):
                ready[h, 2 * n + q] = done[:, q * LANES : (q + 1) * LANES].reshape(POINTS, part, LANES)

        def nearby():
            for step in range(2):
                columns(mate(2 * step) // 2)
                for d in (2 * step, 2 * step + 1):
                    if d > 0:
                        near_send(h, d).start()
                    direct_send(h, d).start()


        def beyond():
            for level in range(2):
                columns(base_far // 2 + level)
            cross(h)

        for stage_of in (nearby, beyond):
            stage_of()
        gathered[h, col, row] = ready[h, row]

    half_rows = lambda start: pl.ds(start, quarter)

    def relay(g, level):
        for f in range(2):
            far_arrival(g, level, f).wait_recv()
            relay_send(g, level, f).start()

    def share_far(g):
        share(spot(g, col, half_rows(base_far)), HALVES + g).start()

    def pass_on(g):
        place = spot(g, across, half_rows(base_far))
        remote(place, place, send_relay, recv_relay.at[g], (row, across)).wait_recv()
        share(place, HALVES + g).start()

    def share_near(h):
        waiter(quarter - 1, send_near, recv_near.at[h]).wait_recv()
        share(gathered.at[h, col, half_rows(base_near)], h).start()
        waiter(quarter, send_direct, recv_direct.at[h]).wait_recv()
        share(gathered.at[h, across, half_rows(base_near)], h).start()

    depth = cols * quarter * part

    def map_out(h, start, points, fresh):
        weights = folded[h, :, half_rows(start)].reshape(depth, -1)
        for k in points:
            spectrum = gathered[h, :, half_rows(start), k].reshape(depth, LANES)
            piece = lax.dot_general(
                spectrum, weights, (((0,), (0,)), ((), ())), preferred_element_type=jnp.float32
            )
            total[k] = piece if fresh else total[k] + piece

    def map_near(h):
        waiter(rows, send_share, recv_share.at[h]).wait_recv()
        map_out(h, base_near, range(POINTS), h == 0)

    def map_far(g):
        h, first, count = groups[g]
        both = gathered.at[h, pl.ds(0, 2), half_rows(base_far), pl.ds(first, count)]
        remote(both, both, send_share, recv_share.at[HALVES + g], (row, sibling)).wait_recv()
        map_out(h, base_far, range(first, first + count), False)

    inner = 1 - outer
    relay(0, outer)
    relay(0, inner)
    share_far(0)
    share_near(0)
    relay(1, outer)
    relay(1, inner)
    relay(2, outer)
    relay(2, inner)
    relay(3, outer)
    relay(3, inner)
    for g in range(1, len(groups)):
        share_far(g)
    pass_on(0)
    map_near(0)
    share_near(1)
    map_far(0)
    pass_on(1)
    map_near(1)
    for g in range(2, len(groups)):
        pass_on(g)
    for g in range(1, len(groups)):
        map_far(g)
    out_ref[...] = jnp.swapaxes(total[...], 0, 1).reshape(out_ref.shape).astype(out_ref.dtype)

    others = pl.ds(0, rows - 1)
    remote(packed.at[:, others], arrived.at[:, others], send_one, recv_one.at[0], (row, sibling)).wait_send()
    waiter(HALVES * len(far), send_far, recv_far.at[0, 0]).wait_send()
    waiter(HALVES * (quarter - 1), send_near, recv_near.at[0]).wait_send()
    waiter(HALVES * quarter, send_direct, recv_direct.at[0]).wait_send()
    waiter(HALVES * len(far), send_relay, recv_relay.at[0]).wait_send()
    everything = gathered.at[0]
    remote(everything, everything, send_share, recv_share.at[0], (row, sibling)).wait_send()


def fused(tokens, norm_gain, w_in, w_out):
    rows, cols = lax.axis_size("row"), lax.axis_size("col")
    block, width_in = tokens.shape
    width = w_in.shape[1]
    features = w_out.shape[1]
    part = width // (HALVES * rows)
    marks = (0, 1, 2, 3, 4, 5, 6, 7, 8)
    forward, fold = channel_tables(width, block * rows)
    twiddles, coarse, fine = position_tables(block, block * rows)
    half, short, wide = jnp.bfloat16, pltpu.VMEM, jnp.float32
    operands = [tokens, norm_gain[None, :], w_in, w_out, forward, fold, twiddles, coarse, fine]
    operands = [pltpu.with_memory_space_constraint(jnp.asarray(x), pltpu.HBM) for x in operands]
    dma = pltpu.SemaphoreType.DMA
    quad = POINTS // 4
    groups = ((0, 0, POINTS), (1, 0, 2 * quad), (1, 2 * quad, quad), (1, 3 * quad, quad))
    return pl.pallas_call(
        functools.partial(mixer_kernel, marks, 4, groups),
        out_shape=jax.ShapeDtypeStruct((block, features), half),
        in_specs=[pl.BlockSpec(memory_space=pl.ANY)] * len(operands),
        out_specs=pl.BlockSpec(memory_space=pltpu.VMEM),
        scratch_shapes=[short(x.shape, x.dtype) for x in operands]
        + [
            short((HALVES, rows, part, block), half),
            short((HALVES, rows, part, block), half),
            short((POINTS, part, 2 * block), half),
            short((2 * block, block), half),
            short((HALVES, rows, POINTS, part, LANES), half),
            short((HALVES, cols, rows, POINTS, part, LANES), half),
            short((HALVES, cols, rows, part, features), half),
            short((POINTS, LANES, features), wide),
            short((width_in, LANES), wide),
            dma((len(marks) - 1,)),
            dma((8,)),
            dma(()),
            dma((HALVES,)),
            dma((5,)),
            dma((HALVES,)),
            dma((len(groups), rows // 2)),
            dma((HALVES,)),
            dma((len(groups),)),
            dma((HALVES + len(groups),)),
        ],
        compiler_params=pltpu.CompilerParams(
            collective_id=0, has_side_effects=True, vmem_limit_bytes=32 * 1024 * 1024
        ),
    )(*operands)


def fits(mesh):
    return mesh.shape["row"] == POINTS and mesh.shape["col"] == 4


def choose(mesh, *arrays):
    tokens, _, w_in, _ = arrays
    group_local = w_in.shape[1] == GROUP
    tiles = tokens.shape[0] == POINTS * LANES
    return fused(*arrays) if fits(mesh) and group_local and tiles else local(*arrays)


def solution(mesh):
    placed = (P("row", None), P(), P(None, "col"), P(None, "col"))
    return jax.shard_map(
        functools.partial(choose, mesh), mesh=mesh, in_specs=placed, out_specs=P("row", "col"), check_vma=False
    )
```
